32 devices in a mesh: ep: 4 (over y, x), tp: 8 (over z, core).
Axes of the slice: x: 2, y: 2, z: 4, core: 2. Of those that a mesh axis runs over, the one named last changes fastest.
Arguments:
- receptance: bfloat16 [4096, 1024], P('ep', 'tp'), may hold values from -6 to 6
- key_in: bfloat16 [4096, 1024], P('ep', 'tp'), may hold values from -6 to 6
- payload_vectors: bfloat16 [4096, 1024], P('ep', 'tp'), may hold values from -6 to 6
- decay_in: bfloat16 [4096, 1024], P('ep', 'tp'), may hold values from -30 to 3
- rate_in: bfloat16 [4096, 1024], P('ep', 'tp'), may hold values from -30 to 6
- gate_in: bfloat16 [4096, 1024], P('ep', 'tp'), may hold values from -6 to 6
- norm_gain: float32 [1024], P('tp'), may hold values from 0.1 to 1.9
- out_weight: bfloat16 [1024, 2048], P('tp'), may hold values from -0.1875 to 0.1875
- moe_in: bfloat16 [4096, 2048], P(('ep', 'tp')), may hold values from -6 to 6
- moe_gain: float32 [2048], replicated, may hold values from 0.1 to 1.9
- routes: int32 [4096, 2], P(('ep', 'tp')), may hold values from 0 to 7, all different within a row; in each aligned block of 128 rows (0 to 127, 128 to 255, ...) at most 48 rows name the same one
- route_weights: float32 [4096, 2], P(('ep', 'tp')), may hold values from 0.2 to 1
- expert_gate: bfloat16 [8, 2048, 512], P('ep', None, 'tp'), may hold values from -0.125 to 0.125
- expert_up: bfloat16 [8, 2048, 512], P('ep', None, 'tp'), may hold values from -0.125 to 0.125
- expert_down: bfloat16 [8, 2048, 512], P('ep', None, 'tp'), may hold values from -0.25 to 0.25
- shared_gate: bfloat16 [2048, 512], replicated, may hold values from -0.125 to 0.125
- shared_up: bfloat16 [2048, 512], replicated, may hold values from -0.125 to 0.125
- shared_down: bfloat16 [512, 2048], replicated, may hold values from -0.25 to 0.25
Outputs:
- mixed: bfloat16 [4096, 2048], P(('ep', 'tp'))
- moe_out: bfloat16 [4096, 2048], P(('ep', 'tp'))
The draws below stay inside these ranges and needn't reach their ends.
Inputs may be any that keep to these rules, and one draw needn't show every extreme that they name: `routes`: each token names 2 different experts; within the rows of one device no expert is named more than 48 times, a bound that some block reaches there.
All inputs are finite; a program needn't handle non-finite values.
Results may differ from the reference program's by a relative error of at most 0.019.
Values may be sent and summed in bfloat16 or wider, within the bound.
A program may use at most 128 MiB of HBM per device.

```python
import math
import jax
import jax.numpy as jnp
import numpy as np
from jax import lax

D = 2048
MIX_WIDTH = 1024
HEAD_DIM = 64
HEADS = 16
BLOCK = 64
SEQ = 4096
MOE_TOKENS = 128
MOE_ALL = 4096
TOP_K = 2
EXPERTS = 8
EXPERT_WIDTH = 512
SHARED_WIDTH = 512
SLOTS = 48


def slow_channel_index(key):
    kinds = jax.random.randint(jax.random.fold_in(key, 11), (HEADS,), 0, 8)
    slow = kinds < 4
    return jnp.repeat(slow, HEAD_DIM)[None, :]


def draw_decay_in(key, part):
    slow = slow_channel_index(key)
    capacity_locations = jnp.arange(SEQ, dtype=jnp.int32)
    noise = jnp.clip(jax.random.normal(jax.random.fold_in(key, 1), (SEQ, MIX_WIDTH), jnp.float32), -2.0, 2.0) * 0.7
    spans = jax.random.uniform(jax.random.fold_in(key, 2), (16,), jnp.float32, -0.7, 0.7)
    shift = spans[capacity_locations * 16 // SEQ][:, None]
    channel = jax.random.uniform(jax.random.fold_in(key, 3), (MIX_WIDTH,), jnp.float32, 0.2, 0.6)[None, :]
    slow_value_rows = jnp.log(channel / SEQ) + 0.5
    fast_value = jnp.log(channel) - 2.6
    displacement_anchor = jnp.where(slow, slow_value_rows, fast_value) + shift + noise
    specialist_places = jax.random.randint(jax.random.fold_in(key, 4), (2,), 0, SEQ)
    contiguous_span_length = jnp.any(capacity_locations[:, None] == specialist_places[None, :], axis=1)[:, None]
    return jnp.where(contiguous_span_length, 1.5, displacement_anchor).astype(jnp.bfloat16)


def draw_rate_in(key, part):
    slow = slow_channel_index(key)
    noise = jnp.clip(jax.random.normal(jax.random.fold_in(key, 5), (SEQ, MIX_WIDTH), jnp.float32), -3.0, 3.0)
    slow_value_rows = jnp.log(jnp.float32(19.2) / SEQ) + 0.7 * noise
    return jnp.where(slow, slow_value_rows, noise).astype(jnp.bfloat16)


def block_scale(rng, shape, shards, least, largest):
    def one(position, shards_of):
        steps = jax.random.uniform(jax.random.fold_in(jax.random.fold_in(rng, 6), position), (shards_of,), jnp.float32, least / len(shards), largest / len(shards))
        return jnp.repeat(jnp.exp(steps), shape[position] // shards_of).reshape((-1,) + (1,) * (len(shape) - position - 1))

    level = one(*shards[0])
    for cut in shards[1:]:
        level = level * one(*cut)
    return level


def shared_out(key, own, number, rows, number_of, top, bound, slope):
    order = jax.random.permutation(key, number_of)
    heavy_load, ordinary = load_shares(number_of, rows * top, bound, slope, True), load_shares(number_of, rows * top, bound, slope, False)
    places = jnp.arange(number_of)

    def named(sizes, offset_by):
        used = int((sizes > 0).sum())
        fixed = max(1, used // 4)
        passed = fixed + (places - fixed + offset_by * (used - fixed)) % max(1, number_of - fixed)
        return jnp.zeros((number_of,), jnp.int32).at[order[jnp.where(places < fixed, places, passed)]].set(jnp.asarray(sizes, jnp.int32))

    sizes = jnp.where(number % 4 == 0, named(heavy_load, number // 4), named(ordinary, number - number // 4 - 1))
    mixed = jax.random.permutation(jax.random.fold_in(own, 3), number_of)
    source_of, receiver = mixed[0:number_of // 2 * 2:2], mixed[1:number_of // 2 * 2:2]
    room = jnp.minimum(sizes[source_of] - 1, bound - sizes[receiver]) // 2
    room = jnp.where((source_of == order[0]) | (receiver == order[0]) | (sizes[receiver] == 0), 0, jnp.maximum(room, 0))
    passed = jax.random.randint(jax.random.fold_in(own, 4), (number_of // 2,), 0, 1 << 20) % (room + 1)
    sizes = sizes.at[source_of].add(-passed).at[receiver].add(passed)
    members = jnp.searchsorted(jnp.cumsum(sizes), jnp.arange(rows * top), side="right").astype(jnp.int32)
    table = members.reshape(top, rows).T
    table = table[jax.random.permutation(jax.random.fold_in(own, 1), rows)]
    offset_by = jax.random.randint(jax.random.fold_in(own, 2), (rows, 1), 0, top)
    return jnp.take_along_axis(table, (jnp.arange(top)[None, :] + offset_by) % top, axis=1)


def load_shares(amount, total, bound, skew, full):
    loads = [(1 << 20) // math.isqrt(standing ** skew) + 1 for standing in range(1, amount + 1)]
    largest = bound if full else min(bound, max(-(-total // amount), total * loads[0] // sum(loads)))
    least = 1 if total - largest >= amount - 1 else 0
    holding, surplus = [largest] + [least] * (amount - 1), total - largest - least * (amount - 1)
    while surplus > 0:
        movable = [i for i in range(1, amount) if holding[i] < largest] or [i for i in range(1, amount) if holding[i] < bound]
        pool, remaining = sum([loads[i] for i in movable]), surplus
        for i in movable:
            more = min(bound - holding[i], max(1, remaining * loads[i] // pool), surplus)
            holding[i] = holding[i] + more
            surplus = surplus - more
    return np.array(holding)


def scatter_about(own_key, dims, width, reach, pieces=(), held_as=jnp.bfloat16):
    factor_of = block_scale(own_key, dims, pieces, -0.22, 0.18) if pieces else 1.0
    entries = jax.random.normal(own_key, dims, jnp.float32) * width * factor_of
    return jnp.minimum(jnp.maximum(entries, -reach), reach).astype(held_as)


def setup_inputs(seed: int = 0) -> dict:
    arg_keys = jax.random.split(jax.random.key(seed), 19)
    receptance = scatter_about(arg_keys[0], (SEQ, MIX_WIDTH), 1.0, 6.0, ((0, 4), (1, 8)))
    key_in = scatter_about(arg_keys[1], (SEQ, MIX_WIDTH), 1.0, 6.0, ((0, 4), (1, 8)))
    payload_vectors = scatter_about(arg_keys[2], (SEQ, MIX_WIDTH), 1.0, 6.0, ((0, 4), (1, 8)))
    decay_in = draw_decay_in(jax.random.fold_in(arg_keys[18], 71), 0)
    rate_in = draw_rate_in(jax.random.fold_in(arg_keys[18], 71), 0)
    gate_in = scatter_about(arg_keys[5], (SEQ, MIX_WIDTH), 1.0, 6.0, ((0, 4), (1, 8)))
    norm_gain = jnp.clip(1.0 + 0.18 * jax.random.normal(arg_keys[6], (MIX_WIDTH,), jnp.float32), 0.1, 1.9)
    out_weight = scatter_about(arg_keys[7], (MIX_WIDTH, D), MIX_WIDTH ** -0.5, 0.1875, ((0, 8),))
    moe_in = scatter_about(arg_keys[8], (MOE_ALL, D), 1.0, 6.0, ((0, 32),))
    moe_gain = jnp.clip(1.0 + 0.18 * jax.random.normal(arg_keys[9], (D,), jnp.float32), 0.1, 1.9)
    routes_keys = jax.random.split(jax.random.fold_in(arg_keys[10], 1), MOE_ALL // MOE_TOKENS)
    routes_turns = jax.random.permutation(jax.random.fold_in(arg_keys[10], 3), MOE_ALL // MOE_TOKENS)
    routes = jax.vmap(lambda own, number: shared_out(jax.random.fold_in(arg_keys[10], 2), own, number, MOE_TOKENS, EXPERTS, TOP_K, SLOTS, 1))(routes_keys, routes_turns).reshape((MOE_ALL, TOP_K))
    route_weights = jnp.clip(0.2 + 0.8 * jax.random.uniform(arg_keys[11], (MOE_ALL, TOP_K), jnp.float32) ** block_scale(arg_keys[11], (MOE_ALL, TOP_K), ((0, 32),), -0.2, 0.2), 0.2, 1.0)
    expert_gate = scatter_about(arg_keys[12], (EXPERTS, D, EXPERT_WIDTH), D ** -0.5, 0.125, ((0, 4), (2, 8)))
    expert_up = scatter_about(arg_keys[13], (EXPERTS, D, EXPERT_WIDTH), D ** -0.5, 0.125, ((0, 4), (2, 8)))
    expert_down = scatter_about(arg_keys[14], (EXPERTS, D, EXPERT_WIDTH), EXPERT_WIDTH ** -0.5, 0.25, ((0, 4), (2, 8)))
    shared_gate = scatter_about(arg_keys[15], (D, SHARED_WIDTH), D ** -0.5, 0.125)
    shared_up = scatter_about(arg_keys[16], (D, SHARED_WIDTH), D ** -0.5, 0.125)
    shared_down = scatter_about(arg_keys[17], (SHARED_WIDTH, D), SHARED_WIDTH ** -0.5, 0.25)
    return {"receptance": receptance, "key_in": key_in, "payload_vectors": payload_vectors, "decay_in": decay_in, "rate_in": rate_in, "gate_in": gate_in, "norm_gain": norm_gain, "out_weight": out_weight, "moe_in": moe_in, "moe_gain": moe_gain, "routes": routes, "route_weights": route_weights, "expert_gate": expert_gate, "expert_up": expert_up, "expert_down": expert_down, "shared_gate": shared_gate, "shared_up": shared_up, "shared_down": shared_down}


def mult(form, left, right):
    return jnp.einsum(form, left, right, precision=lax.Precision.HIGHEST)

def block_maps(receive, keys, values, log_decay, alpha, beta):
    length = receive.shape[-2]
    cumul = jnp.cumsum(log_decay, axis=-2)
    before = cumul - log_decay
    ending = cumul[..., -1:, :]
    query_dec = receive * jnp.exp(cumul)
    alpha_dec = alpha * jnp.exp(before)
    key_grow = keys * jnp.exp(-cumul)
    beta_grow = beta * jnp.exp(-cumul)
    row_index = jnp.arange(length, dtype=jnp.int32)[:, None]
    col_index = jnp.arange(length, dtype=jnp.int32)[None, :]
    strict = col_index < row_index
    inclusive_cumsum = col_index <= row_index
    couple = jnp.where(strict, mult('...tc,...sc->...ts', alpha_dec, beta_grow), 0.0)
    insert_term = jnp.where(strict, mult('...tc,...sc->...ts', alpha_dec, key_grow), 0.0)
    inverse = jnp.eye(length, dtype=jnp.float32) + couple
    power = couple
    for section in range(length.bit_length() - 2):
        power = mult('...ij,...jk->...ik', power, power)
        inverse = inverse + mult('...ij,...jk->...ik', inverse, power)
    q_rows = mult('...ts,...sc->...tc', inverse, alpha_dec)
    z_rows = mult('...ts,...sv->...tv', inverse, mult('...ts,...sv->...tv', insert_term, values))
    read_beta = jnp.where(inclusive_cumsum, mult('...tc,...sc->...ts', query_dec, beta_grow), 0.0)
    read_key = jnp.where(inclusive_cumsum, mult('...tc,...sc->...ts', query_dec, key_grow), 0.0)
    query_bar = query_dec + mult('...ts,...sc->...tc', read_beta, q_rows)
    local_out = mult('...ts,...sv->...tv', read_beta, z_rows) + mult('...ts,...sv->...tv', read_key, values)
    beta_end = beta * jnp.exp(ending - cumul)
    key_end = keys * jnp.exp(ending - cumul)
    eye = jnp.eye(keys.shape[-1], dtype=jnp.float32)
    carry_map = mult('...tc,...td->...cd', q_rows, beta_end) + jnp.exp(ending)[..., 0, :, None] * eye
    source_map = mult('...tv,...tk->...vk', z_rows, beta_end) + mult('...tv,...tk->...vk', values, key_end)
    return (query_bar, local_out, carry_map, source_map)

def mixer(receptance, key_in, payload_vectors, decay_in, rate_in, gate_in, norm_gain, out_weight):
    length = receptance.shape[0]

    def split_heads(array):
        return array.reshape(length // BLOCK, BLOCK, HEADS, HEAD_DIM).transpose(2, 0, 1, 3)
    keys = split_heads(key_in.astype(jnp.float32))
    unit = keys * lax.rsqrt(lax.optimization_barrier(jnp.sum(keys * keys, -1, keepdims=True)) + 1e-06)
    rate = split_heads(jax.nn.sigmoid(rate_in.astype(jnp.float32)))
    log_decay = split_heads(-jnp.exp(-jax.nn.softplus(-decay_in.astype(jnp.float32)) - 0.5))
    queries = split_heads(receptance.astype(jnp.float32))
    values = split_heads(payload_vectors.astype(jnp.float32))

    def one_head(operands):
        query_h, key_h, value_h, decay_h, alpha_h, beta_h = operands
        query_bar, local_out, carry_map, source_map = block_maps(query_h, key_h, value_h, decay_h, alpha_h, beta_h)

        def advance(state, blocks):
            bar_b, local_b, carry_b, source_b = blocks
            output = mult('tk,vk->tv', bar_b, state) + local_b
            return (mult('ij,jk->ik', state, carry_b) + source_b, output)
        start_state = jnp.zeros((HEAD_DIM, HEAD_DIM), jnp.float32)
        final, outputs = lax.scan(advance, start_state, (query_bar, local_out, carry_map, source_map))
        return outputs
    recur = lax.map(one_head, (queries, keys, values, log_decay, -unit, unit * rate))
    recur = recur.transpose(1, 2, 0, 3).reshape(length, HEADS, HEAD_DIM)
    centered = recur - lax.optimization_barrier(jnp.mean(recur, -1, keepdims=True))
    rescaled_input = centered * lax.rsqrt(lax.optimization_barrier(jnp.mean(centered * centered, -1, keepdims=True)) + 0.00064)
    gated = rescaled_input.reshape(length, MIX_WIDTH) * norm_gain * jax.nn.sigmoid(gate_in.astype(jnp.float32))
    mixer_rows = gated.astype(jnp.bfloat16)
    return jnp.dot(mixer_rows, out_weight, preferred_element_type=jnp.float32).astype(jnp.bfloat16)

def experts(moe_in, moe_gain, routes, route_weights, expert_gate, expert_up, expert_down, shared_gate, shared_up, shared_down):
    tile_rows = 128
    values = moe_in.astype(jnp.float32)
    centered = values - lax.optimization_barrier(jnp.mean(values, -1, keepdims=True))
    rescaled_input = (centered * lax.rsqrt(lax.optimization_barrier(jnp.mean(centered * centered, -1, keepdims=True)) + 1e-05) * moe_gain).astype(jnp.bfloat16)
    shared_gate_out = jnp.dot(rescaled_input, shared_gate, preferred_element_type=jnp.float32)
    shared_up_out = jnp.dot(rescaled_input, shared_up, preferred_element_type=jnp.float32)
    shared_hidden = (jax.nn.silu(shared_gate_out) * shared_up_out).astype(jnp.bfloat16)
    shared_term = jnp.dot(shared_hidden, shared_down, preferred_element_type=jnp.float32)
    share = 2.5 * route_weights / lax.optimization_barrier(jnp.sum(route_weights, -1, keepdims=True))
    tokens = rescaled_input.shape[0]
    pairs = tokens * TOP_K
    flat_expert = routes.reshape(-1).astype(jnp.int32)
    flat_token = jnp.repeat(jnp.arange(tokens, dtype=jnp.int32), TOP_K)
    flat_share = share.reshape(-1)
    order = jnp.argsort(flat_expert, stable=True).astype(jnp.int32)
    sorted_expert = flat_expert[order]
    counts = lax.optimization_barrier(jnp.sum((flat_expert[:, None] == jnp.arange(EXPERTS, dtype=jnp.int32)[None, :]).astype(jnp.int32), 0)).astype(jnp.int32)
    padded = ((counts + tile_rows - 1) // tile_rows * tile_rows).astype(jnp.int32)
    pad_end = jnp.cumsum(padded).astype(jnp.int32)
    pad_start = (pad_end - padded).astype(jnp.int32)
    first = (jnp.cumsum(counts) - counts).astype(jnp.int32)
    dest = (pad_start[sorted_expert] + jnp.arange(pairs, dtype=jnp.int32) - first[sorted_expert]).astype(jnp.int32)
    capacity = (pairs + tile_rows - 1) // tile_rows * tile_rows + EXPERTS * tile_rows
    blocks = capacity // tile_rows
    slot_token = jnp.full((capacity,), tokens, jnp.int32).at[dest].set(flat_token[order])
    slot_share = jnp.zeros((capacity,), jnp.float32).at[dest].set(flat_share[order])
    group_starts = jnp.arange(blocks, dtype=jnp.int32) * tile_rows
    block_expert = jnp.minimum(jnp.searchsorted(pad_end, group_starts, side='right').astype(jnp.int32), EXPERTS - 1).astype(jnp.int32)
    rows_padded = jnp.concatenate([rescaled_input, jnp.zeros((1, rescaled_input.shape[1]), jnp.bfloat16)], axis=0)

    def add_block(total, operands):
        token_ids, weights, expert = operands
        rows = rows_padded[token_ids]
        gate = jnp.dot(rows, expert_gate[expert], preferred_element_type=jnp.float32)
        upper = jnp.dot(rows, expert_up[expert], preferred_element_type=jnp.float32)
        hidden = (jax.nn.silu(gate) * upper).astype(jnp.bfloat16)
        result = jnp.dot(hidden, expert_down[expert].T, preferred_element_type=jnp.float32).astype(jnp.bfloat16)
        return (total.at[token_ids].add(result.astype(jnp.float32) * weights[:, None]), None)
    start_total = jnp.zeros((tokens + 1, rescaled_input.shape[1]), jnp.float32)
    total, unused = lax.scan(add_block, start_total, (slot_token.reshape(blocks, tile_rows), slot_share.reshape(blocks, tile_rows), block_expert))
    return (shared_term + total[:tokens]).astype(jnp.bfloat16)

def reference(receptance, key_in, payload_vectors, decay_in, rate_in, gate_in, norm_gain, out_weight, moe_in, moe_gain, routes, route_weights, expert_gate, expert_up, expert_down, shared_gate, shared_up, shared_down):
    mixed = mixer(receptance, key_in, payload_vectors, decay_in, rate_in, gate_in, norm_gain, out_weight)
    moe_out = experts(moe_in, moe_gain, routes, route_weights, expert_gate, expert_up, expert_down, shared_gate, shared_up, shared_down)
    return (mixed, moe_out)
```

```python
import functools

import jax
import jax.numpy as jnp
from jax import lax
from jax.experimental import pallas as pl
from jax.experimental.pallas import tpu as pltpu
from jax.sharding import PartitionSpec as P

HEAD_DIM = 64
BLOCK = 64


def dims(form):
    return {"nn": ((1,), (0,)), "nt": ((1,), (1,)), "tn": ((0,), (0,))}[form]


def mm1(left, right, form="nn"):
    return lax.dot_general(
        left.astype(jnp.bfloat16),
        right.astype(jnp.bfloat16),
        (dims(form), ((), ())),
        preferred_element_type=jnp.float32,
    )


def mm3(left, right, form="nn"):
    lh, rh = left.astype(jnp.bfloat16), right.astype(jnp.bfloat16)
    ll = (left - lh.astype(jnp.float32)).astype(jnp.bfloat16)
    rl = (right - rh.astype(jnp.float32)).astype(jnp.bfloat16)
    return mm1(lh, rh, form) + (mm1(lh, rl, form) + mm1(ll, rh, form))


mm_g = mm3
mm_inv = mm3
mm_q = mm3
mm_out = mm3
mm_car = mm3
mm_scan = mm3


def head_masks(rows, width):
    lane = lax.broadcasted_iota(jnp.int32, (rows, width), 1)
    return lane < HEAD_DIM


def stacked(x):
    first = head_masks(*x.shape)
    return jnp.concatenate([jnp.where(first, x, 0.0), jnp.where(first, 0.0, x)], axis=0)


def per_head_sum(x):
    first = head_masks(*x.shape)
    one = jnp.sum(jnp.where(first, x, 0.0), axis=-1, keepdims=True)
    both = jnp.sum(jnp.where(first, 0.0, x), axis=-1, keepdims=True)
    return jnp.where(first, one, both)


def sigmoid(x):
    return 1.0 / (1.0 + jnp.exp(-x))


def local_block(r_in, k_in, v_in, d_in, b_in):
    f32 = jnp.float32
    keys = k_in.astype(f32)
    unit = keys * lax.rsqrt(per_head_sum(keys * keys) + 1e-06)
    log_decay = sigmoid(d_in.astype(f32)) * -0.6065306597126334
    tri_row = lax.broadcasted_iota(jnp.int32, (BLOCK, 3 * BLOCK), 0)
    tri_col = lax.broadcasted_iota(jnp.int32, (BLOCK, 3 * BLOCK), 1) % BLOCK
    tri = jnp.where(tri_col <= tri_row, 1.0, 0.0).astype(jnp.bfloat16)
    hi = log_decay.astype(jnp.bfloat16)
    rest = log_decay - hi.astype(f32)
    mid = rest.astype(jnp.bfloat16)
    low = (rest - mid.astype(f32)).astype(jnp.bfloat16)
    cumul = mm1(tri, jnp.concatenate([hi, mid, low], axis=0))
    end_scale = jnp.exp(cumul[BLOCK - 1 :, :])
    shrink = jnp.exp(-cumul)
    query2 = stacked(r_in.astype(f32) * jnp.exp(cumul))
    alpha2 = stacked(-unit * jnp.exp(cumul - log_decay))
    key_grow = keys * shrink
    beta_grow = unit * sigmoid(b_in.astype(f32)) * shrink
    values2 = stacked(v_in.astype(f32))
    two = 2 * BLOCK
    grams = mm_g(
        jnp.concatenate([alpha2, query2], axis=0),
        jnp.concatenate([beta_grow, beta_grow, key_grow, key_grow], axis=0),
        "nt",
    )
    row = lax.broadcasted_iota(jnp.int32, (two, two), 0)
    col = lax.broadcasted_iota(jnp.int32, (two, two), 1)
    same = row // BLOCK == col // BLOCK
    strict = same & (col < row)
    inclusive = same & (col <= row)
    couple = jnp.where(strict, grams[:two, :two], 0.0)
    insert = jnp.where(strict, grams[:two, two:], 0.0)
    read_beta = jnp.where(inclusive, grams[two:, :two], 0.0)
    read_key = jnp.where(inclusive, grams[two:, two:], 0.0)
    size = 8
    near = jnp.where(row // size == col // size, couple, 0.0)
    inverse = jnp.where(row == col, 1.0, 0.0) + near
    power = mm_inv(near, near)
    both = mm_inv(jnp.concatenate([inverse, power], axis=0), power)
    inverse = inverse + both[:two]
    inverse = inverse + mm_inv(inverse, both[two:])
    while size < BLOCK:
        wide = 2 * size
        off = jnp.where(
            (row // wide == col // wide) & (row // size != col // size), couple, 0.0
        )
        inverse = inverse + mm_inv(inverse, mm_inv(off, inverse))
        size = wide
    inserted = mm_q(insert, values2)
    qz = mm_q(inverse, jnp.concatenate([alpha2, inserted], axis=1))
    lower = jnp.concatenate([jnp.zeros_like(values2), values2], axis=1)
    stack = jnp.concatenate([qz, lower], axis=0)
    reads = mm_out(jnp.concatenate([read_beta, read_key], axis=1), stack)
    query_bar = query2 + reads[:, :two]
    local_out = reads[:, two:]
    ends = jnp.concatenate([stacked(beta_grow * end_scale), stacked(key_grow * end_scale)], axis=0)
    maps = mm_car(stack, ends, "tn")
    return query_bar, local_out, maps, end_scale


def silu(x):
    return x / (1.0 + jnp.exp(-x))


def layer_kernel(
    unroll,
    pieces,
    slots,
    r_ref,
    k_ref,
    v_ref,
    d_ref,
    b_ref,
    gate_ref,
    gain_ref,
    x_ref,
    moe_gain_ref,
    routes_ref,
    scores_ref,
    project_in,
    expert_gate,
    expert_up,
    expert_down,
    shared_gate,
    shared_up,
    shared_down,
    mixed_ref,
    moe_ref,
    state,
    qp_ref,
    lo_ref,
    rows_ref,
    totals,
    token_ref,
    project,
    weights,
    shared_one,
    shared_two,
    shared_three,
    shared_hidden,
    shared_term,
    others,
    other_routes,
    other_scores,
    normal,
    chosen_ref,
    spread_ref,
    leaving,
    arrived,
    returned,
    hidden_ref,
    part_out,
    part_in,
    token_send,
    token_recv,
    slab_send,
    slab_recv,
    wide_send,
    wide_recv,
    pair_send,
    pair_recv,
    core_send,
    core_recv,
    relay_send,
    relay_recv,
    load_sem,
    go_send,
    go_recv,
    back_send,
    back_recv,
    part_send,
    part_recv,
    ep_send,
    ep_recv,
    row_send,
    row_recv,
):
    f32, bf16 = jnp.float32, jnp.bfloat16
    two = 2 * BLOCK
    MESH = pl.DeviceIdType.MESH
    here, mine = lax.axis_index("ep"), lax.axis_index("tp")
    groups, peers = lax.axis_size("ep"), lax.axis_size("tp")
    depth, core = mine // 2, mine % 2
    teams = peers // 4
    team, side = depth // 2, depth % 2
    seat = side * 2 + core
    facing = (1 - side) * 2 + core
    partner = depth * 2 + 1 - core
    across = team * 4 + facing
    tokens, width = x_ref.shape
    local, height = expert_gate.shape[0], expert_gate.shape[1]
    experts = local * groups
    span = local * slots
    columns = width // groups
    piece = width // pieces
    sources = (expert_gate, expert_up, expert_down)
    kinds = len(sources)

    def remote(source, target, send, recv, device):
        return pltpu.make_async_remote_copy(
            src_ref=source,
            dst_ref=target,
            send_sem=send,
            recv_sem=recv,
            device_id=device,
            device_id_type=MESH,
        )

    def mate(shift):
        return {"tp": (team + shift) % teams * 4 + seat}

    def column(shift):
        return {"ep": (here + groups + shift) % groups}

    def token_copies(s):
        pairs = ((x_ref, others), (routes_ref, other_routes), (scores_ref, other_scores))
        return [
            remote(a, b.at[s], token_send.at[s, i], token_recv.at[s, i], mate(s))
            for i, (a, b) in enumerate(pairs)
        ]

    def slab_place(owner, part):
        return project.at[
            pl.ds(pl.multiple_of(owner * two, two), two),
            pl.ds(pl.multiple_of(part * columns, columns), columns),
        ]

    def slab_copy(s):
        source = project_in.at[:, pl.ds(pl.multiple_of(here * columns, columns), columns)]
        return remote(
            source, slab_place(mine, here), slab_send.at[s], slab_recv.at[s], mate(s)
        )

    def wide_copy(s, q):
        owner = (team + teams - s) % teams * 4 + seat
        block = slab_place(owner, here)
        return remote(block, block, wide_send.at[s, q], wide_recv.at[s, q], column(q))

    def weight_place(a, owner):
        if a < kinds:
            return weights.at[
                pl.ds(a * local, local), pl.ds(pl.multiple_of(owner * height, height), height), :
            ]
        return project_place(0, owner)

    def project_place(s, owner):
        base = (team + teams - s) % teams * 4 + owner
        return project.at[pl.ds(pl.multiple_of(base * two, two), two), :]

    def place_of(a, owner):
        return weight_place(a, owner) if a <= kinds else project_place(a - kinds, owner)

    def own_block(a):
        if a < kinds:
            return sources[a]
        return project_in if a == kinds else project_place(a - kinds, seat)

    def pair_copy(a):
        return remote(
            own_block(a), place_of(a, seat), pair_send.at[a], pair_recv.at[a], {"tp": across}
        )

    def core_copy(a):
        return remote(
            own_block(a), place_of(a, seat), core_send.at[a], core_recv.at[a], {"tp": partner}
        )

    def relay_copy(a):
        block = place_of(a, facing)
        return remote(block, block, relay_send.at[a], relay_recv.at[a], {"tp": partner})

    def own_copy(a):
        return pltpu.make_async_copy(own_block(a), place_of(a, seat), load_sem.at[a])

    def relay(a):
        pair_copy(a).wait_recv()
        relay_copy(a).start()

    def ready(a):
        core_copy(a).wait_recv()
        relay_copy(a).wait_recv()

    def shared_copy(i):
        source = (shared_gate, shared_up, shared_down)[i]
        target = (shared_one, shared_two, shared_three)[i]
        return pltpu.make_async_copy(source, target, load_sem.at[kinds + 1 + i])

    def go_copy(s, q):
        return remote(
            leaving.at[s, q], arrived.at[s, q], go_send.at[s, q], go_recv.at[s, q], column(q)
        )

    def back_copy(s, q, n):
        cols = pl.ds(pl.multiple_of(n * piece, piece), piece)
        return remote(
            arrived.at[s, q, :, cols],
            returned.at[s, q, :, cols],
            back_send.at[s, q, n],
            back_recv.at[s, q, n],
            column(-q),
        )

    def part_copy(s, n):
        cols = pl.ds(pl.multiple_of(n * piece, piece), piece)
        return remote(
            part_out.at[s, :, cols],
            part_in.at[s, :, cols],
            part_send.at[s, n],
            part_recv.at[s, n],
            mate(teams - s),
        )

    barrier = pltpu.get_barrier_semaphore()
    for q in range(1, peers):
        pl.semaphore_signal(
            barrier, inc=1, device_id={"tp": (mine + q) % peers}, device_id_type=MESH
        )
    for q in range(1, groups):
        pl.semaphore_signal(
            barrier, inc=1, device_id={"ep": (here + q) % groups}, device_id_type=MESH
        )
    pl.semaphore_wait(barrier, peers + groups - 2)

    for s in range(1, teams):
        for copy in token_copies(s):
            copy.start()
    for a in range(kinds + 1):
        pair_copy(a).start()
        core_copy(a).start()
        own_copy(a).start()
    for s in range(1, teams):
        slab_copy(s).start()
    for i in range(3):
        shared_copy(i).start()

    def normalize(source, target):
        tall = 16

        def some(i, carry):
            rows = pl.ds(pl.multiple_of(i * tall, tall), tall)
            values = source[rows, :].astype(f32)
            centered = values - jnp.sum(values, -1, keepdims=True) * (1.0 / width)
            spread = jnp.sum(centered * centered, -1, keepdims=True) * (1.0 / width)
            target[rows, :] = (centered * lax.rsqrt(spread + 1e-05) * moe_gain_ref[...]).astype(
                bf16
            )
            return carry

        lax.fori_loop(0, tokens // tall, some, 0)

    def dispatch(s, source, routes, scores, held):
        normalize(source, normal.at[held])
        count = max(16, experts)
        order = lax.broadcasted_iota(jnp.int32, (count, tokens), 0)
        names = (here + order // local) % groups * local + order % local
        names = jnp.where(order < experts, names, -1)
        tops = routes.shape[0]
        hits = [routes[k : k + 1, :] == names for k in range(tops)]
        picks = sum(jnp.where(hit, 1.0, 0.0) for hit in hits)
        past = lax.broadcasted_iota(jnp.int32, (tokens, tokens), 0)
        present = lax.broadcasted_iota(jnp.int32, (tokens, tokens), 1)
        earlier = mm1(picks, jnp.where(past < present, 1.0, 0.0))
        index = order.astype(f32) * slots + earlier
        row = lax.broadcasted_iota(jnp.int32, (experts * slots, tokens), 0).astype(f32)
        match = [
            row == jnp.sum(jnp.where(hit, index, 0.0), axis=0, keepdims=True) for hit in hits
        ]
        total = sum(scores[k : k + 1, :] for k in range(tops))
        chosen_ref[...] = sum(jnp.where(m, 1.0, 0.0) for m in match).astype(bf16)
        spread = sum(
            jnp.where(match[k], 2.5 * scores[k : k + 1, :] / total, 0.0) for k in range(tops)
        )
        spread_ref[s] = jnp.transpose(spread).astype(bf16)
        step = 256

        def fill(i, carry):
            cols = pl.ds(pl.multiple_of(i * step, step), step)
            out = jnp.dot(
                chosen_ref[...], normal[held, :, cols], preferred_element_type=f32
            ).astype(bf16)
            arrived[s, 0, :, cols] = out[:span]
            leaving[s, 1:, :, cols] = out[span:].reshape(groups - 1, span, step)
            return carry

        lax.fori_loop(0, width // step, fill, 0)

        def send(q, carry):
            go_copy(s, q).start()
            return carry

        lax.fori_loop(1, groups, send, 0)

    dispatch(0, x_ref, routes_ref, scores_ref, 0)

    row = lax.broadcasted_iota(jnp.int32, (2 * two, two), 0)
    col = lax.broadcasted_iota(jnp.int32, (2 * two, two), 1)
    state[...] = jnp.where(row == col, 1.0, 0.0)
    turns = r_ref.shape[0] // (BLOCK * unroll)

    def turn(step, carry):
        parts = []
        for u in range(unroll):
            rows = pl.ds(pl.multiple_of((step * unroll + u) * BLOCK, BLOCK), BLOCK)
            parts.append(
                local_block(
                    r_ref[rows, :], k_ref[rows, :], v_ref[rows, :], d_ref[rows, :], b_ref[rows, :]
                )
            )
        now = state[...]
        for u, (query_bar, local_out, maps, end_scale) in enumerate(parts):
            rows = pl.ds(pl.multiple_of((step * unroll + u) * BLOCK, BLOCK), BLOCK)
            out = mm_scan(query_bar, now, "nt")
            qp_ref[rows, :] = out[:BLOCK, :two] + out[BLOCK:, :two]
            lo = out[:, two:] + local_out
            lo_ref[rows, :] = lo[:BLOCK] + lo[BLOCK:]
            moved = mm_scan(now, maps[:two]) + now * end_scale
            now = jnp.concatenate([moved[:two], moved[two:] + maps[two:]], axis=0)
        state[...] = now
        return carry

    lax.fori_loop(0, turns, turn, 0)

    carry_map, source_map = state[:two, :], state[two:, :]
    totals[here, 0] = (carry_map[:BLOCK] + carry_map[BLOCK:]).astype(totals.dtype)
    totals[here, 1] = (source_map[:BLOCK] + source_map[BLOCK:]).astype(totals.dtype)

    def ep_copy(q, slot):
        return remote(
            totals.at[slot], totals.at[slot], ep_send.at[q], ep_recv.at[q], column(q)
        )

    for q in range(1, groups):
        ep_copy(q, here).start()

    relay(0)

    def receive(s, carry):
        for copy in token_copies(s):
            copy.wait_recv()
        dispatch(s, others.at[s], other_routes.at[s], other_scores.at[s], 1)
        slab_copy(s).wait_recv()

        def widen(q, inner):
            wide_copy(s, q).start()
            return inner

        lax.fori_loop(1, groups, widen, 0)
        return carry

    lax.fori_loop(1, teams, receive, 0)

    for i in range(3):
        shared_copy(i).wait()
    step = 256
    for i in range(shared_one.shape[1] // step):
        cols = slice(i * step, (i + 1) * step)
        gate = jnp.dot(normal[0], shared_one[:, cols], preferred_element_type=f32)
        upper = jnp.dot(normal[0], shared_two[:, cols], preferred_element_type=f32)
        shared_hidden[:, cols] = (silu(gate) * upper).astype(bf16)

    def share(i, carry):
        cols = pl.ds(pl.multiple_of(i * step, step), step)
        shared_term[:, cols] = jnp.dot(
            shared_hidden[...], shared_three[:, cols], preferred_element_type=f32
        )
        return carry

    lax.fori_loop(0, width // step, share, 0)

    for q in range(1, groups):
        ep_copy(q, (here + groups - q) % groups).wait_recv()

    def enter(k, entry):
        carry = stacked(totals[k, 0].astype(f32))
        source = stacked(totals[k, 1].astype(f32))
        reached = jnp.where(k < here, 1.0, 0.0)
        return entry + reached * (mm3(entry, carry) + source - entry)

    entry = lax.fori_loop(0, groups, enter, jnp.zeros((two, two), f32))

    def row_copy(q, target, source):
        return remote(
            rows_ref.at[pl.ds(pl.multiple_of(target * tokens, tokens), tokens), :],
            token_ref.at[:, pl.ds(pl.multiple_of(source * two, two), two)],
            row_send.at[q],
            row_recv.at[q],
            {"tp": target},
        )

    def finish(rows):
        recur = mm3(qp_ref[rows, :], entry, "nt") + lo_ref[rows, :]
        centered = recur - per_head_sum(recur) * (1.0 / HEAD_DIM)
        spread = per_head_sum(centered * centered) * (1.0 / HEAD_DIM)
        normed = centered * lax.rsqrt(spread + 0.00064)
        gated = normed * gain_ref[...] * sigmoid(gate_ref[rows, :].astype(f32))
        rows_ref[rows, :] = gated.astype(bf16)

    def finish_turn(q, carry):
        finish(pl.ds(pl.multiple_of(q * tokens, tokens), tokens))
        return carry

    lax.fori_loop(0, peers, finish_turn, 0)
    own_rows = pltpu.make_async_copy(
        rows_ref.at[pl.ds(pl.multiple_of(mine * tokens, tokens), tokens), :],
        token_ref.at[:, pl.ds(pl.multiple_of(mine * two, two), two)],
        load_sem.at[kinds + 4],
    )
    own_rows.start()

    def row_start(q, carry):
        row_copy(q, (mine + q) % peers, mine).start()
        return carry

    lax.fori_loop(1, peers, row_start, 0)

    for a in range(1, kinds):
        relay(a)
    for a in range(kinds):
        own_copy(a).wait()
        ready(a)
    nt = (((1,), (1,)), ((), ()))

    def feed(i, carry):
        s = (i + 1) % teams

        def come(q, inner):
            go_copy(s, q).wait_recv()
            return inner

        lax.fori_loop(1, groups, come, 0)
        for e in range(local):
            mine_slots = slice(e * slots, (e + 1) * slots)
            x = arrived[s, :, mine_slots, :].reshape(groups * slots, width)
            gate = lax.dot_general(x, weights[e], nt, preferred_element_type=f32)
            upper = lax.dot_general(x, weights[local + e], nt, preferred_element_type=f32)
            hidden_ref[e] = (silu(gate) * upper).astype(bf16)

        def down(n, inner):
            cols = pl.ds(pl.multiple_of(n * piece, piece), piece)
            for e in range(local):
                mine_slots = slice(e * slots, (e + 1) * slots)
                out = jnp.dot(
                    hidden_ref[e], weights[2 * local + e, :, cols], preferred_element_type=f32
                )
                out = out.astype(bf16).reshape(groups, slots, piece)
                returned[s, 0, mine_slots, cols] = out[0]
                arrived[s, 1:, mine_slots, cols] = out[1:]

            def back(q, last):
                back_copy(s, q, n).start()
                return last

            return lax.fori_loop(1, groups, back, inner)

        return lax.fori_loop(0, pieces, down, carry)

    lax.fori_loop(0, teams, feed, 0)

    relay(kinds)
    for s in range(1, teams):

        def widened(q, carry, s=s):
            wide_copy(s, q).wait_recv()
            return carry

        lax.fori_loop(1, groups, widened, 0)
        pair_copy(kinds + s).start()
        core_copy(kinds + s).start()

    def combined(s, n):
        def come(q, carry):
            back_copy(s, q, n).wait_recv()
            return carry

        lax.fori_loop(1, groups, come, 0)
        cols = pl.ds(pl.multiple_of(n * piece, piece), piece)
        rows = returned[s, :, :, cols].reshape(groups * span, piece)
        return jnp.dot(spread_ref[s], rows, preferred_element_type=f32), cols

    def partial(s, carry):
        def some(n, inner):
            value, cols = combined(s, n)
            part_out[s, :, cols] = value.astype(bf16)
            part_copy(s, n).start()
            return inner

        return lax.fori_loop(0, pieces, some, carry)

    lax.fori_loop(1, teams, partial, 0)

    for a in range(kinds + 1, kinds + teams):
        relay(a)
    own_copy(kinds).wait()
    for a in range(kinds, kinds + teams):
        ready(a)
    own_rows.wait()

    def row_end(q, carry):
        row_copy(q, (mine + q) % peers, (mine + peers - q) % peers).wait()
        return carry

    lax.fori_loop(1, peers, row_end, 0)

    def mix(i, carry):
        cols = pl.ds(pl.multiple_of(i * step, step), step)
        mixed_ref[:, cols] = jnp.dot(
            token_ref[...], project[:, cols], preferred_element_type=f32
        ).astype(bf16)
        return carry

    lax.fori_loop(0, width // step, mix, 0)

    def close(n, carry):
        value, cols = combined(0, n)
        total = value + shared_term[:, cols]
        for s in range(1, teams):
            part_copy(s, n).wait_recv()
            total = total + part_in[s, :, cols].astype(f32)
        moe_ref[:, cols] = total.astype(bf16)
        return carry

    lax.fori_loop(0, pieces, close, 0)

    for a in range(kinds + teams):
        pair_copy(a).wait_send()
        core_copy(a).wait_send()
        relay_copy(a).wait_send()
    for q in range(1, groups):
        ep_copy(q, here).wait_send()

    def sent(s, carry):
        def each(q, inner):
            go_copy(s, q).wait_send()

            def block(n, last):
                back_copy(s, q, n).wait_send()
                return last

            return lax.fori_loop(0, pieces, block, inner)

        return lax.fori_loop(1, groups, each, carry)

    lax.fori_loop(0, teams, sent, 0)

    def shipped(s, carry):
        for copy in token_copies(s):
            copy.wait_send()
        slab_copy(s).wait_send()

        def each(q, inner):
            wide_copy(s, q).wait_send()
            return inner

        def block(n, inner):
            part_copy(s, n).wait_send()
            return inner

        lax.fori_loop(1, groups, each, 0)
        return lax.fori_loop(0, pieces, block, carry)

    lax.fori_loop(1, teams, shipped, 0)


def shards(
    receptance,
    key_in,
    payload_vectors,
    decay_in,
    rate_in,
    gate_in,
    norm_gain,
    out_weight,
    moe_in,
    moe_gain,
    routes,
    route_weights,
    expert_gate,
    expert_up,
    expert_down,
    shared_gate,
    shared_up,
    shared_down,
):
    length, channels = receptance.shape
    tokens, width = moe_in.shape
    groups, peers = lax.axis_size("ep"), lax.axis_size("tp")
    teams = peers // 4
    local, _, height = expert_gate.shape
    top_count = routes.shape[1]
    experts = local * groups
    slots = max(2, 3 * tokens * top_count // (2 * experts))
    slots = -(-slots // 16) * 16
    span = local * slots
    inner = shared_gate.shape[1]
    pieces = 4
    kinds = 3
    wide = 2 * HEAD_DIM
    spare = wide - channels
    pad = lambda x: jnp.pad(x, ((0, 0),) * (x.ndim - 1) + ((0, spare),)) if spare else x
    weight_rows = jnp.pad(out_weight, ((0, spare), (0, 0))) if spare else out_weight
    f32, bf16 = jnp.float32, jnp.bfloat16
    vmem = pl.BlockSpec(memory_space=pltpu.VMEM)
    anywhere = pl.BlockSpec(memory_space=pl.ANY)
    dma = pltpu.SemaphoreType.DMA
    out = jax.ShapeDtypeStruct((tokens, width), bf16)
    turned = lambda w: jnp.swapaxes(w, 1, 2)
    return pl.pallas_call(
        functools.partial(layer_kernel, 4, pieces, slots),
        out_shape=(out, out),
        in_specs=[vmem] * 11 + [anywhere] * 7,
        out_specs=(vmem, vmem),
        scratch_shapes=[
            pltpu.VMEM((2 * wide, wide), f32),
            pltpu.VMEM((length, wide), f32),
            pltpu.VMEM((length, wide), f32),
            pltpu.VMEM((length, wide), bf16),
            pltpu.VMEM((groups, 2, HEAD_DIM, wide), bf16),
            pltpu.VMEM((tokens, peers * wide), bf16),
            pltpu.VMEM((peers * wide, width), bf16),
            pltpu.VMEM((kinds * local, 4 * height, width), bf16),
            pltpu.VMEM(shared_gate.shape, bf16),
            pltpu.VMEM(shared_up.shape, bf16),
            pltpu.VMEM(shared_down.shape, bf16),
            pltpu.VMEM((tokens, inner), bf16),
            pltpu.VMEM((tokens, width), f32),
            pltpu.VMEM((teams, tokens, width), bf16),
            pltpu.VMEM((teams, top_count, tokens), jnp.int32),
            pltpu.VMEM((teams, top_count, tokens), f32),
            pltpu.VMEM((2, tokens, width), bf16),
            pltpu.VMEM((experts * slots, tokens), bf16),
            pltpu.VMEM((teams, tokens, experts * slots), bf16),
            pltpu.VMEM((teams, groups, span, width), bf16),
            pltpu.VMEM((teams, groups, span, width), bf16),
            pltpu.VMEM((teams, groups, span, width), bf16),
            pltpu.VMEM((local, groups * slots, 4 * height), bf16),
            pltpu.VMEM((teams, tokens, width), bf16),
            pltpu.VMEM((teams, tokens, width), bf16),
            dma((teams, 3)),
            dma((teams, 3)),
            dma((teams,)),
            dma((teams,)),
            dma((teams, groups)),
            dma((teams, groups)),
            dma((kinds + teams,)),
            dma((kinds + teams,)),
            dma((kinds + teams,)),
            dma((kinds + teams,)),
            dma((kinds + teams,)),
            dma((kinds + teams,)),
            dma((kinds + 5,)),
            dma((teams, groups)),
            dma((teams, groups)),
            dma((teams, groups, pieces)),
            dma((teams, groups, pieces)),
            dma((teams, pieces)),
            dma((teams, pieces)),
            dma((groups,)),
            dma((groups,)),
            dma((peers,)),
            dma((peers,)),
        ],
        compiler_params=pltpu.CompilerParams(
            collective_id=0, has_side_effects=True, vmem_limit_bytes=63 << 20
        ),
    )(
        pad(receptance),
        pad(key_in),
        pad(payload_vectors),
        pad(decay_in),
        pad(rate_in),
        pad(gate_in),
        pad(norm_gain).reshape(1, wide),
        moe_in,
        moe_gain.reshape(1, width),
        routes.T,
        route_weights.T,
        weight_rows,
        turned(expert_gate),
        turned(expert_up),
        turned(expert_down),
        shared_gate,
        shared_up,
        shared_down,
    )


def solution(mesh):
    placed = (
        P("ep", "tp"),
        P("ep", "tp"),
        P("ep", "tp"),
        P("ep", "tp"),
        P("ep", "tp"),
        P("ep", "tp"),
        P("tp"),
        P("tp", None),
        P(("ep", "tp"), None),
        P(),
        P(("ep", "tp"), None),
        P(("ep", "tp"), None),
        P("ep", None, "tp"),
        P("ep", None, "tp"),
        P("ep", None, "tp"),
        P(),
        P(),
        P(),
    )
    return jax.shard_map(
        shards,
        mesh=mesh,
        in_specs=placed,
        out_specs=(P(("ep", "tp"), None), P(("ep", "tp"), None)),
        check_vma=False,
    )
```

```python
import functools

import jax
import jax.numpy as jnp
from jax import lax
from jax.experimental import pallas as pl
from jax.experimental.pallas import tpu as pltpu
from jax.sharding import PartitionSpec as P

HEAD_DIM = 64
BLOCK = 64


def dims(form):
    return {"nn": ((1,), (0,)), "nt": ((1,), (1,)), "tn": ((0,), (0,))}[form]


def mm1(left, right, form="nn"):
    return lax.dot_general(
        left.astype(jnp.bfloat16),
        right.astype(jnp.bfloat16),
        (dims(form), ((), ())),
        preferred_element_type=jnp.float32,
    )


def mm3(left, right, form="nn"):
    lh, rh = left.astype(jnp.bfloat16), right.astype(jnp.bfloat16)
    ll = (left - lh.astype(jnp.float32)).astype(jnp.bfloat16)
    rl = (right - rh.astype(jnp.float32)).astype(jnp.bfloat16)
    return mm1(lh, rh, form) + (mm1(lh, rl, form) + mm1(ll, rh, form))


mm_g = mm1
mm_inv = mm1
mm_q = mm1
mm_out = mm1
mm_car = mm1
mm_scan = mm1
mm_step = mm1
mm_fin = mm1


def head_masks(rows, width):
    lane = lax.broadcasted_iota(jnp.int32, (rows, width), 1)
    return lane < HEAD_DIM


def stacked(x):
    first = head_masks(*x.shape)
    return jnp.concatenate([jnp.where(first, x, 0.0), jnp.where(first, 0.0, x)], axis=0)


def per_head_sum(x):
    first = head_masks(*x.shape)
    one = jnp.sum(jnp.where(first, x, 0.0), axis=-1, keepdims=True)
    both = jnp.sum(jnp.where(first, 0.0, x), axis=-1, keepdims=True)
    return jnp.where(first, one, both)


def sigmoid(x):
    return 1.0 / (1.0 + jnp.exp(-x))


def block_stages(r_in, k_in, v_in, d_in, b_in):
    f32 = jnp.float32
    keys = k_in.astype(f32)
    unit = keys * lax.rsqrt(per_head_sum(keys * keys) + 1e-06)
    log_decay = sigmoid(d_in.astype(f32)) * -0.6065306597126334
    tri_row = lax.broadcasted_iota(jnp.int32, (BLOCK, 3 * BLOCK), 0)
    tri_col = lax.broadcasted_iota(jnp.int32, (BLOCK, 3 * BLOCK), 1) % BLOCK
    tri = jnp.where(tri_col <= tri_row, 1.0, 0.0).astype(jnp.bfloat16)
    hi = log_decay.astype(jnp.bfloat16)
    rest = log_decay - hi.astype(f32)
    mid = rest.astype(jnp.bfloat16)
    low = (rest - mid.astype(f32)).astype(jnp.bfloat16)
    cumul = mm1(tri, jnp.concatenate([hi, mid, low], axis=0))
    yield
    end_scale = jnp.exp(cumul[BLOCK - 1 :, :])
    shrink = jnp.exp(-cumul)
    query = r_in.astype(f32) * jnp.exp(cumul)
    alpha = -unit * jnp.exp(cumul - log_decay)
    key_grow = keys * shrink
    beta_grow = unit * sigmoid(b_in.astype(f32)) * shrink
    values = v_in.astype(f32)
    values2 = stacked(values)
    two = 2 * BLOCK
    grams = mm_g(
        jnp.concatenate([alpha, query], axis=0),
        jnp.concatenate([stacked(beta_grow), stacked(key_grow)], axis=0),
        "nt",
    )
    yield
    row = lax.broadcasted_iota(jnp.int32, (BLOCK, two), 0)
    col = lax.broadcasted_iota(jnp.int32, (BLOCK, two), 1) % BLOCK
    strict = col < row
    inclusive = col <= row
    couple = jnp.where(strict, grams[:BLOCK, :two], 0.0)
    insert = jnp.where(strict, grams[:BLOCK, two:], 0.0)
    read_beta = jnp.where(inclusive, grams[BLOCK:, :two], 0.0)
    read_key = jnp.where(inclusive, grams[BLOCK:, two:], 0.0)
    size = 8
    near = jnp.where(row // size == col // size, couple, 0.0)
    inverse = jnp.where(row == col, 1.0, 0.0) + near
    power = mm_inv(near, stacked(near))
    yield
    both = mm_inv(jnp.concatenate([inverse, power], axis=0), stacked(power))
    yield
    inverse = inverse + both[:BLOCK]
    inverse = inverse + mm_inv(inverse, stacked(both[BLOCK:]))
    yield
    while size < BLOCK:
        wide = 2 * size
        off = jnp.where(
            (row // wide == col // wide) & (row // size != col // size), couple, 0.0
        )
        step = mm_inv(off, stacked(inverse))
        yield
        inverse = inverse + mm_inv(inverse, stacked(step))
        yield
        size = wide
    inserted = mm_q(insert, values2)
    yield
    qz = mm_q(inverse, jnp.concatenate([stacked(alpha), stacked(inserted)], axis=1))
    yield
    q_rows, z_rows = qz[:, :two], qz[:, two:]
    upper = jnp.concatenate([stacked(q_rows), stacked(z_rows)], axis=1)
    lower = jnp.concatenate([jnp.zeros_like(values2), values2], axis=1)
    reads = mm_out(
        jnp.concatenate([read_beta, read_key], axis=1), jnp.concatenate([upper, lower], axis=0)
    )
    yield
    query_bar = query + reads[:, :two]
    local_out = reads[:, two:]
    ends = jnp.concatenate([beta_grow * end_scale, key_grow * end_scale], axis=0)
    lower = jnp.concatenate([jnp.zeros_like(values), values], axis=1)
    maps = mm_car(ends, jnp.concatenate([qz, lower], axis=0), "tn")
    yield
    head_row = lax.broadcasted_iota(jnp.int32, (two, 2 * two), 0) // HEAD_DIM
    head_col = lax.broadcasted_iota(jnp.int32, (two, 2 * two), 1) % two // HEAD_DIM
    maps = jnp.where(head_row == head_col, maps, 0.0)
    row = lax.broadcasted_iota(jnp.int32, (two, two), 0)
    col = lax.broadcasted_iota(jnp.int32, (two, two), 1)
    fade = jnp.sum(jnp.where(row == col, end_scale, 0.0), axis=1, keepdims=True)
    return query_bar, local_out, maps, fade


def local_blocks(inputs):
    stages = [block_stages(*block) for block in inputs]
    results = [None] * len(stages)
    while None in results:
        for i, stage in enumerate(stages):
            try:
                next(stage)
            except StopIteration as end:
                results[i] = end.value
    return results


def silu(x):
    return x / (1.0 + jnp.exp(-x))


def layer_kernel(
    unroll,
    pieces,
    slots,
    gain_ref,
    x_ref,
    moe_gain_ref,
    routes_ref,
    scores_ref,
    r_in,
    k_in,
    v_in,
    d_in,
    b_in,
    gate_in,
    project_in,
    expert_gate,
    expert_up,
    expert_down,
    shared_gate,
    shared_up,
    shared_down,
    mixed_ref,
    moe_ref,
    streams,
    state,
    qp_ref,
    lo_ref,
    rows_ref,
    totals,
    token_ref,
    project,
    weights,
    shared_one,
    shared_two,
    shared_three,
    shared_hidden,
    shared_term,
    others,
    other_routes,
    other_scores,
    normal,
    chosen_ref,
    spread_ref,
    leaving,
    arrived,
    returned,
    hidden_ref,
    part_out,
    part_in,
    table_send,
    table_recv,
    token_send,
    token_recv,
    slab_send,
    slab_recv,
    wide_send,
    wide_recv,
    pair_send,
    pair_recv,
    core_send,
    core_recv,
    relay_send,
    relay_recv,
    load_sem,
    stream_sem,
    go_send,
    go_recv,
    back_send,
    back_recv,
    part_send,
    part_recv,
    ep_send,
    ep_recv,
    row_send,
    row_recv,
):
    f32, bf16 = jnp.float32, jnp.bfloat16
    two = 2 * BLOCK
    MESH = pl.DeviceIdType.MESH
    stream_copies = [
        pltpu.make_async_copy(source, streams.at[i], stream_sem.at[i])
        for i, source in enumerate((r_in, k_in, v_in, d_in, b_in, gate_in))
    ]
    for copy in stream_copies:
        copy.start()
    here, mine = lax.axis_index("ep"), lax.axis_index("tp")
    groups, peers = lax.axis_size("ep"), lax.axis_size("tp")
    depth, core = mine // 2, mine % 2
    teams = peers // 4
    team, side = depth // 2, depth % 2
    seat = side * 2 + core
    facing = (1 - side) * 2 + core
    partner = depth * 2 + 1 - core
    across = team * 4 + facing
    tokens, width = x_ref.shape
    local, height = expert_gate.shape[0], expert_gate.shape[1]
    experts = local * groups
    span = local * slots
    columns = width // groups
    piece = width // pieces
    sources = (expert_gate, expert_up, expert_down)
    kinds = len(sources)
    cuts = kinds * local

    def remote(source, target, send, recv, device):
        return pltpu.make_async_remote_copy(
            src_ref=source,
            dst_ref=target,
            send_sem=send,
            recv_sem=recv,
            device_id=device,
            device_id_type=MESH,
        )

    def mate(shift):
        return {"tp": (team + shift) % teams * 4 + seat}

    def column(shift):
        return {"ep": (here + groups + shift) % groups}

    def table_copies(s):
        pairs = ((routes_ref, other_routes), (scores_ref, other_scores))
        return [
            remote(a, b.at[s], table_send.at[s, i], table_recv.at[s, i], mate(s))
            for i, (a, b) in enumerate(pairs)
        ]

    def token_copy(s, n):
        cols = pl.ds(pl.multiple_of(n * piece, piece), piece)
        return remote(
            normal.at[:, cols],
            others.at[s, :, cols],
            token_send.at[s, n],
            token_recv.at[s, n],
            mate(s),
        )

    def slab_place(owner, part):
        return project.at[
            pl.ds(pl.multiple_of(owner * two, two), two),
            pl.ds(pl.multiple_of(part * columns, columns), columns),
        ]

    def slab_copy(s):
        source = project_in.at[:, pl.ds(pl.multiple_of(here * columns, columns), columns)]
        target = mate(s) if s else {"tp": across}
        return remote(source, slab_place(mine, here), slab_send.at[s], slab_recv.at[s], target)

    def wide_copy(s, q):
        owner = (team + teams - s) % teams * 4 + seat if s else across
        block = slab_place(owner, here)
        return remote(block, block, wide_send.at[s, q], wide_recv.at[s, q], column(q))

    def weight_place(a, owner):
        return weights.at[a, pl.ds(pl.multiple_of(owner * height, height), height), :]

    def project_place(s, owner):
        base = (team + teams - s) % teams * 4 + owner
        return project.at[pl.ds(pl.multiple_of(base * two, two), two), :]

    def place_of(a, owner):
        return weight_place(a, owner) if a < cuts else project_place(a - cuts, owner)

    def own_block(a):
        if a < cuts:
            return sources[a % kinds].at[a // kinds]
        return project_in if a == cuts else project_place(a - cuts, seat)

    def pair_copy(a):
        return remote(
            own_block(a), place_of(a, seat), pair_send.at[a], pair_recv.at[a], {"tp": across}
        )

    def core_copy(a):
        return remote(
            own_block(a), place_of(a, seat), core_send.at[a], core_recv.at[a], {"tp": partner}
        )

    def relay_copy(a):
        block = place_of(a, facing)
        return remote(block, block, relay_send.at[a], relay_recv.at[a], {"tp": partner})

    def own_copy(a):
        return pltpu.make_async_copy(own_block(a), place_of(a, seat), load_sem.at[a])

    def relay(a):
        pair_copy(a).wait_recv()
        relay_copy(a).start()

    def ready(a):
        core_copy(a).wait_recv()
        relay_copy(a).wait_recv()

    def shared_copy(i):
        source = (shared_gate, shared_up, shared_down)[i]
        target = (shared_one, shared_two, shared_three)[i]
        return pltpu.make_async_copy(source, target, load_sem.at[cuts + 1 + i])

    def go_copy(s, q, n):
        cols = pl.ds(pl.multiple_of(n * piece, piece), piece)
        return remote(
            leaving.at[s, q, :, cols],
            arrived.at[s, q, :, cols],
            go_send.at[s, q, n],
            go_recv.at[s, q, n],
            column(q),
        )

    def back_copy(s, e, q, n):
        cols = pl.ds(pl.multiple_of(n * piece, piece), piece)
        return remote(
            arrived.at[s, q, pl.ds(e * slots, slots), cols],
            returned.at[s, q, pl.ds(e * slots, slots), cols],
            back_send.at[s, e, q, n],
            back_recv.at[s, e, q, n],
            column(-q),
        )

    def part_copy(s, n):
        cols = pl.ds(pl.multiple_of(n * piece, piece), piece)
        return remote(
            part_out.at[s, :, cols],
            part_in.at[s, :, cols],
            part_send.at[s, n],
            part_recv.at[s, n],
            mate(teams - s),
        )

    barrier = pltpu.get_barrier_semaphore()
    for q in range(1, peers):
        pl.semaphore_signal(
            barrier, inc=1, device_id={"tp": (mine + q) % peers}, device_id_type=MESH
        )
    for q in range(1, groups):
        pl.semaphore_signal(
            barrier, inc=1, device_id={"ep": (here + q) % groups}, device_id_type=MESH
        )
    def normalize():
        tall = 16

        def some(i, carry):
            rows = pl.ds(pl.multiple_of(i * tall, tall), tall)
            values = x_ref[rows, :].astype(f32)
            centered = values - jnp.sum(values, -1, keepdims=True) * (1.0 / width)
            spread = jnp.sum(centered * centered, -1, keepdims=True) * (1.0 / width)
            normal[rows, :] = (centered * lax.rsqrt(spread + 1e-05) * moe_gain_ref[...]).astype(
                bf16
            )
            return carry

        lax.fori_loop(0, tokens // tall, some, 0)

    def prepare(s, routes, scores):
        count = max(16, experts)
        order = lax.broadcasted_iota(jnp.int32, (count, tokens), 0)
        names = (here + order // local) % groups * local + order % local
        names = jnp.where(order < experts, names, -1)
        tops = routes.shape[0]
        hits = [routes[k : k + 1, :] == names for k in range(tops)]
        picks = sum(jnp.where(hit, 1.0, 0.0) for hit in hits)
        past = lax.broadcasted_iota(jnp.int32, (tokens, tokens), 0)
        present = lax.broadcasted_iota(jnp.int32, (tokens, tokens), 1)
        earlier = mm1(picks, jnp.where(past < present, 1.0, 0.0))
        index = order.astype(f32) * slots + earlier
        row = lax.broadcasted_iota(jnp.int32, (experts * slots, tokens), 0).astype(f32)
        match = [
            row == jnp.sum(jnp.where(hit, index, 0.0), axis=0, keepdims=True) for hit in hits
        ]
        total = sum(scores[k : k + 1, :] for k in range(tops))
        chosen_ref[...] = sum(jnp.where(m, 1.0, 0.0) for m in match).astype(bf16)
        spread = sum(
            jnp.where(match[k], 2.5 * scores[k : k + 1, :] / total, 0.0) for k in range(tops)
        )
        spread_ref[s] = jnp.transpose(spread).astype(bf16)

    def dispatch(s, n, source):
        half = piece // 2
        for i in range(2):
            cols = pl.ds(pl.multiple_of(n * piece + i * half, half), half)
            out = jnp.dot(chosen_ref[...], source[:, cols], preferred_element_type=f32).astype(bf16)
            arrived[s, 0, :, cols] = out[:span]
            leaving[s, 1:, :, cols] = out[span:].reshape(groups - 1, span, half)

        def send(q, carry):
            go_copy(s, q, n).start()
            return carry

        lax.fori_loop(1, groups, send, 0)

    normalize()
    prepare(0, routes_ref, scores_ref)
    pl.semaphore_wait(barrier, peers + groups - 2)

    for s in range(1, teams):
        for copy in table_copies(s):
            copy.start()
        for n in range(pieces):
            token_copy(s, n).start()
    for s in range(teams):
        slab_copy(s).start()
    for a in range(cuts + 1):
        if a < cuts:
            pair_copy(a).start()
        core_copy(a).start()
        own_copy(a).start()
    for i in range(3):
        shared_copy(i).start()

    def own_piece(n, carry):
        dispatch(0, n, normal)
        return carry

    lax.fori_loop(0, pieces, own_piece, 0)
    for copy in stream_copies:
        copy.wait()
    r_ref, k_ref, v_ref, d_ref, b_ref, gate_ref = (streams.at[i] for i in range(6))

    row = lax.broadcasted_iota(jnp.int32, (two, 2 * two), 0)
    col = lax.broadcasted_iota(jnp.int32, (two, 2 * two), 1)
    state[...] = jnp.where(row == col, 1.0, 0.0)
    turns = r_ref.shape[0] // (BLOCK * unroll)

    def turn(step, carry):
        places = [
            pl.ds(pl.multiple_of((step * unroll + u) * BLOCK, BLOCK), BLOCK) for u in range(unroll)
        ]
        parts = local_blocks(
            [[ref[rows, :] for ref in (r_ref, k_ref, v_ref, d_ref, b_ref)] for rows in places]
        )
        now = state[...]
        for rows, (query_bar, local_out, maps, fade) in zip(places, parts):
            out = mm_scan(query_bar, now)
            qp_ref[rows, :] = out[:, :two]
            lo_ref[rows, :] = out[:, two:] + local_out
            moved = mm_step(maps[:, :two], now) + now * fade
            now = jnp.concatenate([moved[:, :two], moved[:, two:] + maps[:, two:]], axis=1)
        state[...] = now
        return carry

    lax.fori_loop(0, turns, turn, 0)

    carry_map, source_map = state[:, :two], state[:, two:]
    totals[here, 0] = (carry_map[:BLOCK] + carry_map[BLOCK:]).astype(totals.dtype)
    totals[here, 1] = (source_map[:BLOCK] + source_map[BLOCK:]).astype(totals.dtype)

    def ep_copy(q, slot):
        return remote(
            totals.at[slot], totals.at[slot], ep_send.at[q], ep_recv.at[q], column(q)
        )

    for q in range(1, groups):
        ep_copy(q, here).start()

    def widen(s):
        slab_copy(s).wait_recv()

        def each(q, carry):
            wide_copy(s, q).start()
            return carry

        lax.fori_loop(1, groups, each, 0)

    def widened(s):
        def each(q, carry):
            wide_copy(s, q).wait_recv()
            return carry

        lax.fori_loop(1, groups, each, 0)

    def receive(s, carry):
        for copy in table_copies(s):
            copy.wait_recv()
        prepare(s, other_routes.at[s], other_scores.at[s])

        def other_piece(n, inner):
            token_copy(s, n).wait_recv()
            dispatch(s, n, others.at[s])
            return inner

        return lax.fori_loop(0, pieces, other_piece, carry)

    lax.fori_loop(1, teams, receive, 0)

    for s in range(teams):
        widen(s)

    for i in range(3):
        shared_copy(i).wait()
    step = 256
    for i in range(shared_one.shape[1] // step):
        cols = slice(i * step, (i + 1) * step)
        gate = jnp.dot(normal[...], shared_one[:, cols], preferred_element_type=f32)
        upper = jnp.dot(normal[...], shared_two[:, cols], preferred_element_type=f32)
        shared_hidden[:, cols] = (silu(gate) * upper).astype(bf16)

    def share(i, carry):
        cols = pl.ds(pl.multiple_of(i * step, step), step)
        shared_term[:, cols] = jnp.dot(
            shared_hidden[...], shared_three[:, cols], preferred_element_type=f32
        )
        return carry

    lax.fori_loop(0, width // step, share, 0)

    for q in range(1, groups):
        ep_copy(q, (here + groups - q) % groups).wait_recv()

    def enter(k, entry):
        carry = stacked(totals[k, 0].astype(f32))
        source = stacked(totals[k, 1].astype(f32))
        reached = jnp.where(k < here, 1.0, 0.0)
        return entry + reached * (mm3(carry, entry) + source - entry)

    entry = lax.fori_loop(0, groups, enter, jnp.zeros((two, two), f32))

    def row_copy(q, target, source):
        return remote(
            rows_ref.at[pl.ds(pl.multiple_of(target * tokens, tokens), tokens), :],
            token_ref.at[:, pl.ds(pl.multiple_of(source * two, two), two)],
            row_send.at[q],
            row_recv.at[q],
            {"tp": target},
        )

    def finish(rows):
        recur = mm_fin(qp_ref[rows, :], entry) + lo_ref[rows, :]
        centered = recur - per_head_sum(recur) * (1.0 / HEAD_DIM)
        spread = per_head_sum(centered * centered) * (1.0 / HEAD_DIM)
        normed = centered * lax.rsqrt(spread + 0.00064)
        gated = normed * gain_ref[...] * sigmoid(gate_ref[rows, :].astype(f32))
        rows_ref[rows, :] = gated.astype(bf16)

    def finish_turn(q, carry):
        finish(pl.ds(pl.multiple_of(q * tokens, tokens), tokens))
        return carry

    lax.fori_loop(0, peers, finish_turn, 0)
    own_rows = pltpu.make_async_copy(
        rows_ref.at[pl.ds(pl.multiple_of(mine * tokens, tokens), tokens), :],
        token_ref.at[:, pl.ds(pl.multiple_of(mine * two, two), two)],
        load_sem.at[cuts + 4],
    )
    own_rows.start()

    def row_start(q, carry):
        row_copy(q, (mine + q) % peers, mine).start()
        return carry

    lax.fori_loop(1, peers, row_start, 0)

    nt = (((1,), (1,)), ((), ()))

    def feed(s, e):
        mine_slots = pl.ds(e * slots, slots)
        x = arrived[s, :, mine_slots, :].reshape(groups * slots, width)
        gate = lax.dot_general(x, weights[e * kinds], nt, preferred_element_type=f32)
        upper = lax.dot_general(x, weights[e * kinds + 1], nt, preferred_element_type=f32)
        hidden_ref[...] = (silu(gate) * upper).astype(bf16)

        def down(n, carry):
            cols = pl.ds(pl.multiple_of(n * piece, piece), piece)
            out = jnp.dot(
                hidden_ref[...], weights[e * kinds + 2, :, cols], preferred_element_type=f32
            )
            out = out.astype(bf16).reshape(groups, slots, piece)
            returned[s, 0, mine_slots, cols] = out[0]
            arrived[s, 1:, mine_slots, cols] = out[1:]

            def back(q, inner):
                back_copy(s, e, q, n).start()
                return inner

            return lax.fori_loop(1, groups, back, carry)

        lax.fori_loop(0, pieces, down, 0)

    def come(s):
        def each(q, carry):
            def some(n, inner):
                go_copy(s, q, n).wait_recv()
                return inner

            return lax.fori_loop(0, pieces, some, carry)

        lax.fori_loop(1, groups, each, 0)

    def have(e):
        for a in range(e * kinds, (e + 1) * kinds):
            relay(a)
        for a in range(e * kinds, (e + 1) * kinds):
            own_copy(a).wait()
            ready(a)

    for e in range(local):
        have(e)

        def mates(s, carry, e=e):
            if e == 0:
                come(s)
            feed(s, e)
            return carry

        lax.fori_loop(1, teams, mates, 0)
        if e == 0:
            for s in range(1, teams):
                widened(s)
                pair_copy(cuts + s).start()
                core_copy(cuts + s).start()
            widened(0)
            relay_copy(cuts).start()
    come(0)

    def mine_too(e, carry):
        feed(0, e)
        return carry

    lax.fori_loop(0, local, mine_too, 0)

    def combined(s, n):
        def each(q, carry):
            for e in range(local):
                back_copy(s, e, q, n).wait_recv()
            return carry

        lax.fori_loop(1, groups, each, 0)
        cols = pl.ds(pl.multiple_of(n * piece, piece), piece)
        rows = returned[s, :, :, cols].reshape(groups * span, piece)
        return jnp.dot(spread_ref[s], rows, preferred_element_type=f32), cols

    def partial(s, carry):
        def some(n, inner):
            value, cols = combined(s, n)
            part_out[s, :, cols] = value.astype(bf16)
            part_copy(s, n).start()
            return inner

        return lax.fori_loop(0, pieces, some, carry)

    lax.fori_loop(1, teams, partial, 0)

    for a in range(cuts + 1, cuts + teams):
        relay(a)
    own_copy(cuts).wait()
    for a in range(cuts, cuts + teams):
        ready(a)
    own_rows.wait()

    def row_end(q, carry):
        row_copy(q, (mine + q) % peers, (mine + peers - q) % peers).wait()
        return carry

    lax.fori_loop(1, peers, row_end, 0)

    def mix(i, carry):
        cols = pl.ds(pl.multiple_of(i * step, step), step)
        mixed_ref[:, cols] = jnp.dot(
            token_ref[...], project[:, cols], preferred_element_type=f32
        ).astype(bf16)
        return carry

    lax.fori_loop(0, width // step, mix, 0)

    def close(n, carry):
        value, cols = combined(0, n)
        total = value + shared_term[:, cols]
        for s in range(1, teams):
            part_copy(s, n).wait_recv()
            total = total + part_in[s, :, cols].astype(f32)
        moe_ref[:, cols] = total.astype(bf16)
        return carry

    lax.fori_loop(0, pieces, close, 0)

    for a in range(cuts + teams):
        if a != cuts:
            pair_copy(a).wait_send()
        core_copy(a).wait_send()
        relay_copy(a).wait_send()
    for q in range(1, groups):
        ep_copy(q, here).wait_send()

    def sent(s, carry):
        def each(q, inner):
            def block(n, last):
                go_copy(s, q, n).wait_send()
                for e in range(local):
                    back_copy(s, e, q, n).wait_send()
                return last

            return lax.fori_loop(0, pieces, block, inner)

        return lax.fori_loop(1, groups, each, carry)

    lax.fori_loop(0, teams, sent, 0)

    def shipped(s, carry):
        for copy in table_copies(s):
            copy.wait_send()

        def block(n, inner):
            part_copy(s, n).wait_send()
            token_copy(s, n).wait_send()
            return inner

        return lax.fori_loop(0, pieces, block, carry)

    lax.fori_loop(1, teams, shipped, 0)
    for s in range(teams):
        slab_copy(s).wait_send()

        def spread_out(q, carry, s=s):
            wide_copy(s, q).wait_send()
            return carry

        lax.fori_loop(1, groups, spread_out, 0)


def shards(
    receptance,
    key_in,
    payload_vectors,
    decay_in,
    rate_in,
    gate_in,
    norm_gain,
    out_weight,
    moe_in,
    moe_gain,
    routes,
    route_weights,
    expert_gate,
    expert_up,
    expert_down,
    shared_gate,
    shared_up,
    shared_down,
):
    length, channels = receptance.shape
    tokens, width = moe_in.shape
    groups, peers = lax.axis_size("ep"), lax.axis_size("tp")
    teams = peers // 4
    local, _, height = expert_gate.shape
    top_count = routes.shape[1]
    experts = local * groups
    slots = max(2, 3 * tokens * top_count // (2 * experts))
    slots = -(-slots // 16) * 16
    span = local * slots
    inner = shared_gate.shape[1]
    pieces = 4
    kinds = 3
    wide = 2 * HEAD_DIM
    spare = wide - channels
    pad = lambda x: jnp.pad(x, ((0, 0),) * (x.ndim - 1) + ((0, spare),)) if spare else x
    weight_rows = jnp.pad(out_weight, ((0, spare), (0, 0))) if spare else out_weight
    f32, bf16 = jnp.float32, jnp.bfloat16
    vmem = pl.BlockSpec(memory_space=pltpu.VMEM)
    anywhere = pl.BlockSpec(memory_space=pl.ANY)
    dma = pltpu.SemaphoreType.DMA
    out = jax.ShapeDtypeStruct((tokens, width), bf16)
    turned = lambda w: jnp.swapaxes(w, 1, 2)
    return pl.pallas_call(
        functools.partial(layer_kernel, 8, pieces, slots),
        out_shape=(out, out),
        in_specs=[vmem] * 5 + [anywhere] * 13,
        out_specs=(vmem, vmem),
        scratch_shapes=[
            pltpu.VMEM((6, length, wide), bf16),
            pltpu.VMEM((wide, 2 * wide), f32),
            pltpu.VMEM((length, wide), f32),
            pltpu.VMEM((length, wide), f32),
            pltpu.VMEM((length, wide), bf16),
            pltpu.VMEM((groups, 2, HEAD_DIM, wide), bf16),
            pltpu.VMEM((tokens, peers * wide), bf16),
            pltpu.VMEM((peers * wide, width), bf16),
            pltpu.VMEM((kinds * local, 4 * height, width), bf16),
            pltpu.VMEM(shared_gate.shape, bf16),
            pltpu.VMEM(shared_up.shape, bf16),
            pltpu.VMEM(shared_down.shape, bf16),
            pltpu.VMEM((tokens, inner), bf16),
            pltpu.VMEM((tokens, width), f32),
            pltpu.VMEM((teams, tokens, width), bf16),
            pltpu.VMEM((teams, top_count, tokens), jnp.int32),
            pltpu.VMEM((teams, top_count, tokens), f32),
            pltpu.VMEM((tokens, width), bf16),
            pltpu.VMEM((experts * slots, tokens), bf16),
            pltpu.VMEM((teams, tokens, experts * slots), bf16),
            pltpu.VMEM((teams, groups, span, width), bf16),
            pltpu.VMEM((teams, groups, span, width), bf16),
            pltpu.VMEM((teams, groups, span, width), bf16),
            pltpu.VMEM((groups * slots, 4 * height), bf16),
            pltpu.VMEM((teams, tokens, width), bf16),
            pltpu.VMEM((teams, tokens, width), bf16),
            dma((teams, 2)),
            dma((teams, 2)),
            dma((teams, pieces)),
            dma((teams, pieces)),
            dma((teams,)),
            dma((teams,)),
            dma((teams, groups)),
            dma((teams, groups)),
            dma((kinds * local + teams,)),
            dma((kinds * local + teams,)),
            dma((kinds * local + teams,)),
            dma((kinds * local + teams,)),
            dma((kinds * local + teams,)),
            dma((kinds * local + teams,)),
            dma((kinds * local + 5,)),
            dma((6,)),
            dma((teams, groups, pieces)),
            dma((teams, groups, pieces)),
            dma((teams, local, groups, pieces)),
            dma((teams, local, groups, pieces)),
            dma((teams, pieces)),
            dma((teams, pieces)),
            dma((groups,)),
            dma((groups,)),
            dma((peers,)),
            dma((peers,)),
        ],
        compiler_params=pltpu.CompilerParams(
            collective_id=0, has_side_effects=True, vmem_limit_bytes=63 << 20
        ),
    )(
        pad(norm_gain).reshape(1, wide),
        moe_in,
        moe_gain.reshape(1, width),
        routes.T,
        route_weights.T,
        pad(receptance),
        pad(key_in),
        pad(payload_vectors),
        pad(decay_in),
        pad(rate_in),
        pad(gate_in),
        weight_rows,
        turned(expert_gate),
        turned(expert_up),
        turned(expert_down),
        shared_gate,
        shared_up,
        shared_down,
    )


def solution(mesh):
    placed = (
        P("ep", "tp"),
        P("ep", "tp"),
        P("ep", "tp"),
        P("ep", "tp"),
        P("ep", "tp"),
        P("ep", "tp"),
        P("tp"),
        P("tp", None),
        P(("ep", "tp"), None),
        P(),
        P(("ep", "tp"), None),
        P(("ep", "tp"), None),
        P("ep", None, "tp"),
        P("ep", None, "tp"),
        P("ep", None, "tp"),
        P(),
        P(),
        P(),
    )
    return jax.shard_map(
        shards,
        mesh=mesh,
        in_specs=placed,
        out_specs=(P(("ep", "tp"), None), P(("ep", "tp"), None)),
        check_vma=False,
    )
```

```python
import functools

import jax
import jax.numpy as jnp
from jax import lax
from jax.experimental import pallas as pl
from jax.experimental.pallas import tpu as pltpu
from jax.sharding import PartitionSpec as P

HEAD_DIM = 64
BLOCK = 64


def dims(form):
    return {"nn": ((1,), (0,)), "nt": ((1,), (1,)), "tn": ((0,), (0,))}[form]


def mm1(left, right, form="nn"):
    return lax.dot_general(
        left.astype(jnp.bfloat16),
        right.astype(jnp.bfloat16),
        (dims(form), ((), ())),
        preferred_element_type=jnp.float32,
    )


def mm3(left, right, form="nn"):
    lh, rh = left.astype(jnp.bfloat16), right.astype(jnp.bfloat16)
    ll = (left - lh.astype(jnp.float32)).astype(jnp.bfloat16)
    rl = (right - rh.astype(jnp.float32)).astype(jnp.bfloat16)
    return mm1(lh, rh, form) + (mm1(lh, rl, form) + mm1(ll, rh, form))


mm_g = mm1
mm_inv = mm1
mm_q = mm1
mm_out = mm1
mm_car = mm1
mm_scan = mm1
mm_step = mm1
mm_fin = mm1


def head_masks(rows, width):
    lane = lax.broadcasted_iota(jnp.int32, (rows, width), 1)
    return lane < HEAD_DIM


def stacked(x):
    first = head_masks(*x.shape)
    return jnp.concatenate([jnp.where(first, x, 0.0), jnp.where(first, 0.0, x)], axis=0)


def per_head_sum(x):
    first = head_masks(*x.shape)
    one = jnp.sum(jnp.where(first, x, 0.0), axis=-1, keepdims=True)
    both = jnp.sum(jnp.where(first, 0.0, x), axis=-1, keepdims=True)
    return jnp.where(first, one, both)


def sigmoid(x):
    return 1.0 / (1.0 + jnp.exp(-x))


def block_stages(r_in, k_in, v_in, d_in, b_in):
    f32 = jnp.float32
    keys = k_in.astype(f32)
    unit = keys * lax.rsqrt(per_head_sum(keys * keys) + 1e-06)
    log_decay = sigmoid(d_in.astype(f32)) * -0.6065306597126334
    tri_row = lax.broadcasted_iota(jnp.int32, (BLOCK, 3 * BLOCK), 0)
    tri_col = lax.broadcasted_iota(jnp.int32, (BLOCK, 3 * BLOCK), 1) % BLOCK
    tri = jnp.where(tri_col <= tri_row, 1.0, 0.0).astype(jnp.bfloat16)
    hi = log_decay.astype(jnp.bfloat16)
    rest = log_decay - hi.astype(f32)
    mid = rest.astype(jnp.bfloat16)
    low = (rest - mid.astype(f32)).astype(jnp.bfloat16)
    cumul = mm1(tri, jnp.concatenate([hi, mid, low], axis=0))
    yield
    end_scale = jnp.exp(cumul[BLOCK - 1 :, :])
    shrink = jnp.exp(-cumul)
    query = r_in.astype(f32) * jnp.exp(cumul)
    alpha = -unit * jnp.exp(cumul - log_decay)
    key_grow = keys * shrink
    beta_grow = unit * sigmoid(b_in.astype(f32)) * shrink
    values = v_in.astype(f32)
    values2 = stacked(values)
    two = 2 * BLOCK
    grams = mm_g(
        jnp.concatenate([alpha, query], axis=0),
        jnp.concatenate([stacked(beta_grow), stacked(key_grow)], axis=0),
        "nt",
    )
    yield
    row = lax.broadcasted_iota(jnp.int32, (BLOCK, two), 0)
    col = lax.broadcasted_iota(jnp.int32, (BLOCK, two), 1) % BLOCK
    strict = col < row
    inclusive = col <= row
    couple = jnp.where(strict, grams[:BLOCK, :two], 0.0)
    insert = jnp.where(strict, grams[:BLOCK, two:], 0.0)
    read_beta = jnp.where(inclusive, grams[BLOCK:, :two], 0.0)
    read_key = jnp.where(inclusive, grams[BLOCK:, two:], 0.0)
    size = 8
    near = jnp.where(row // size == col // size, couple, 0.0)
    inverse = jnp.where(row == col, 1.0, 0.0) + near
    power = mm_inv(near, stacked(near))
    yield
    both = mm_inv(jnp.concatenate([inverse, power], axis=0), stacked(power))
    yield
    inverse = inverse + both[:BLOCK]
    inverse = inverse + mm_inv(inverse, stacked(both[BLOCK:]))
    yield
    while size < BLOCK:
        wide = 2 * size
        off = jnp.where(
            (row // wide == col // wide) & (row // size != col // size), couple, 0.0
        )
        step = mm_inv(off, stacked(inverse))
        yield
        inverse = inverse + mm_inv(inverse, stacked(step))
        yield
        size = wide
    inserted = mm_q(insert, values2)
    yield
    qz = mm_q(inverse, jnp.concatenate([stacked(alpha), stacked(inserted)], axis=1))
    yield
    q_rows, z_rows = qz[:, :two], qz[:, two:]
    upper = jnp.concatenate([stacked(q_rows), stacked(z_rows)], axis=1)
    lower = jnp.concatenate([jnp.zeros_like(values2), values2], axis=1)
    reads = mm_out(
        jnp.concatenate([read_beta, read_key], axis=1), jnp.concatenate([upper, lower], axis=0)
    )
    yield
    query_bar = query + reads[:, :two]
    local_out = reads[:, two:]
    ends = jnp.concatenate([beta_grow * end_scale, key_grow * end_scale], axis=0)
    lower = jnp.concatenate([jnp.zeros_like(values), values], axis=1)
    maps = mm_car(ends, jnp.concatenate([qz, lower], axis=0), "tn")
    yield
    head_row = lax.broadcasted_iota(jnp.int32, (two, 2 * two), 0) // HEAD_DIM
    head_col = lax.broadcasted_iota(jnp.int32, (two, 2 * two), 1) % two // HEAD_DIM
    maps = jnp.where(head_row == head_col, maps, 0.0)
    row = lax.broadcasted_iota(jnp.int32, (two, two), 0)
    col = lax.broadcasted_iota(jnp.int32, (two, two), 1)
    fade = jnp.sum(jnp.where(row == col, end_scale, 0.0), axis=1, keepdims=True)
    return query_bar, local_out, maps, fade


def local_blocks(inputs):
    stages = [block_stages(*block) for block in inputs]
    results = [None] * len(stages)
    while None in results:
        for i, stage in enumerate(stages):
            try:
                next(stage)
            except StopIteration as end:
                results[i] = end.value
    return results


def silu(x):
    return x / (1.0 + jnp.exp(-x))


def layer_kernel(
    unroll,
    pieces,
    slots,
    gain_in,
    x_in,
    moe_gain_in,
    routes_in,
    scores_in,
    r_in,
    k_in,
    v_in,
    d_in,
    b_in,
    gate_in,
    project_in,
    expert_gate,
    expert_up,
    expert_down,
    shared_gate,
    shared_up,
    shared_down,
    mixed_ref,
    moe_ref,
    x_ref,
    moe_gain_ref,
    routes_ref,
    scores_ref,
    gain_ref,
    streams,
    state,
    qp_ref,
    lo_ref,
    rows_ref,
    totals,
    token_ref,
    project,
    weights,
    downs,
    shared_one,
    shared_two,
    shared_three,
    shared_hidden,
    shared_term,
    others,
    other_routes,
    other_scores,
    normal,
    chosen_ref,
    spread_ref,
    leaving,
    arrived,
    returned,
    hidden_ref,
    part_out,
    part_in,
    table_send,
    table_recv,
    token_send,
    token_recv,
    slab_send,
    slab_recv,
    wide_send,
    wide_recv,
    pair_send,
    pair_recv,
    core_send,
    core_recv,
    relay_send,
    relay_recv,
    load_sem,
    stream_sem,
    go_send,
    go_recv,
    back_send,
    back_recv,
    part_send,
    part_recv,
    ep_send,
    ep_recv,
    row_send,
    row_recv,
):
    f32, bf16 = jnp.float32, jnp.bfloat16
    two = 2 * BLOCK
    MESH = pl.DeviceIdType.MESH
    first_pairs = (
        (x_in, x_ref),
        (moe_gain_in, moe_gain_ref),
        (routes_in, routes_ref),
        (scores_in, scores_ref),
        (gain_in, gain_ref),
    )
    first_copies = [
        pltpu.make_async_copy(source, target, stream_sem.at[6 + i])
        for i, (source, target) in enumerate(first_pairs)
    ]
    stream_copies = [
        pltpu.make_async_copy(source, streams.at[i], stream_sem.at[i])
        for i, source in enumerate((r_in, k_in, v_in, d_in, b_in, gate_in))
    ]
    for copy in first_copies + stream_copies:
        copy.start()
    here, mine = lax.axis_index("ep"), lax.axis_index("tp")
    groups, peers = lax.axis_size("ep"), lax.axis_size("tp")
    depth, core = mine // 2, mine % 2
    teams = peers // 4
    team, side = depth // 2, depth % 2
    seat = side * 2 + core
    facing = (1 - side) * 2 + core
    partner = depth * 2 + 1 - core
    across = team * 4 + facing
    tokens, width = x_in.shape
    local, height = expert_gate.shape[0], expert_gate.shape[1]
    experts = local * groups
    span = local * slots
    columns = width // groups
    piece = width // pieces
    sources = (expert_gate, expert_up)
    firsts = 2 * local
    cuts = firsts + pieces

    def remote(source, target, send, recv, device):
        return pltpu.make_async_remote_copy(
            src_ref=source,
            dst_ref=target,
            send_sem=send,
            recv_sem=recv,
            device_id=device,
            device_id_type=MESH,
        )

    def mate(shift):
        return {"tp": (team + shift) % teams * 4 + seat}

    def column(shift):
        return {"ep": (here + groups + shift) % groups}

    def table_copies(s):
        pairs = ((routes_ref, other_routes), (scores_ref, other_scores))
        return [
            remote(a, b.at[s], table_send.at[s, i], table_recv.at[s, i], mate(s))
            for i, (a, b) in enumerate(pairs)
        ]

    def token_copy(s, n):
        cols = pl.ds(pl.multiple_of(n * piece, piece), piece)
        return remote(
            normal.at[:, cols],
            others.at[s, :, cols],
            token_send.at[s, n],
            token_recv.at[s, n],
            mate(s),
        )

    def slab_place(owner, part):
        return project.at[
            pl.ds(pl.multiple_of(owner * two, two), two),
            pl.ds(pl.multiple_of(part * columns, columns), columns),
        ]

    def slab_copy(s):
        source = project_in.at[:, pl.ds(pl.multiple_of(here * columns, columns), columns)]
        target = mate(s) if s else {"tp": across}
        return remote(source, slab_place(mine, here), slab_send.at[s], slab_recv.at[s], target)

    bits = groups.bit_length() - 1

    def flipped(mask):
        place = here
        for i in range(bits):
            if mask >> i & 1:
                place = place + (1 << i) * (1 - here // (1 << i) % 2 * 2)
        return place

    def wide_copy(s, k, j):
        owner = (team + teams - s) % teams * 4 + seat if s else across
        order = [(i + s) % bits for i in range(bits)]
        mask = sum((j >> i & 1) << order[i] for i in range(k))
        block = slab_place(owner, flipped(mask))
        slot = (1 << k) + j
        target = {"ep": flipped(1 << order[k])}
        return remote(block, block, wide_send.at[s, slot], wide_recv.at[s, slot], target)

    def wide_copies(s, k):
        return [wide_copy(s, k, j) for j in range(1 << k)]

    def weight_place(a, owner):
        rows = pl.ds(pl.multiple_of(owner * height, height), height)
        if a < firsts:
            return weights.at[a, rows, :]
        return downs.at[:, rows, pl.ds((a - firsts) * piece, piece)]

    def project_place(s, owner):
        base = (team + teams - s) % teams * 4 + owner
        return project.at[pl.ds(pl.multiple_of(base * two, two), two), :]

    def place_of(a, owner):
        return weight_place(a, owner) if a < cuts else project_place(a - cuts, owner)

    def own_block(a):
        if a < firsts:
            return sources[a % 2].at[a // 2]
        if a < cuts:
            return expert_down.at[:, :, pl.ds((a - firsts) * piece, piece)]
        return project_in if a == cuts else project_place(a - cuts, seat)

    def pair_copy(a):
        return remote(
            own_block(a), place_of(a, seat), pair_send.at[a], pair_recv.at[a], {"tp": across}
        )

    def core_copy(a):
        return remote(
            own_block(a), place_of(a, seat), core_send.at[a], core_recv.at[a], {"tp": partner}
        )

    def relay_copy(a):
        block = place_of(a, facing)
        return remote(block, block, relay_send.at[a], relay_recv.at[a], {"tp": partner})

    def own_copy(a):
        return pltpu.make_async_copy(own_block(a), place_of(a, seat), load_sem.at[a])

    def relay(a):
        pair_copy(a).wait_recv()
        relay_copy(a).start()

    def ready(a):
        core_copy(a).wait_recv()
        relay_copy(a).wait_recv()

    def shared_copy(i):
        source = (shared_gate, shared_up, shared_down)[i]
        target = (shared_one, shared_two, shared_three)[i]
        return pltpu.make_async_copy(source, target, load_sem.at[cuts + 1 + i])

    def go_copy(s, q, n):
        cols = pl.ds(pl.multiple_of(n * piece, piece), piece)
        return remote(
            leaving.at[s, q, :, cols],
            arrived.at[s, q, :, cols],
            go_send.at[s, q, n],
            go_recv.at[s, q, n],
            column(q),
        )

    def back_copy(s, q, n):
        cols = pl.ds(pl.multiple_of(n * piece, piece), piece)
        return remote(
            arrived.at[s, q, :, cols],
            returned.at[s, q, :, cols],
            back_send.at[s, q, n],
            back_recv.at[s, q, n],
            column(-q),
        )

    def part_copy(s, n):
        cols = pl.ds(pl.multiple_of(n * piece, piece), piece)
        return remote(
            part_out.at[s, :, cols],
            part_in.at[s, :, cols],
            part_send.at[s, n],
            part_recv.at[s, n],
            mate(teams - s),
        )

    barrier = pltpu.get_barrier_semaphore()
    for q in range(1, peers):
        pl.semaphore_signal(
            barrier, inc=1, device_id={"tp": (mine + q) % peers}, device_id_type=MESH
        )
    for q in range(1, groups):
        pl.semaphore_signal(
            barrier, inc=1, device_id={"ep": (here + q) % groups}, device_id_type=MESH
        )
    def normalize():
        tall = 16

        def some(i, carry):
            rows = pl.ds(pl.multiple_of(i * tall, tall), tall)
            values = x_ref[rows, :].astype(f32)
            centered = values - jnp.sum(values, -1, keepdims=True) * (1.0 / width)
            spread = jnp.sum(centered * centered, -1, keepdims=True) * (1.0 / width)
            normal[rows, :] = (centered * lax.rsqrt(spread + 1e-05) * moe_gain_ref[...]).astype(
                bf16
            )
            return carry

        lax.fori_loop(0, tokens // tall, some, 0)

    def prepare(s, routes, scores):
        count = max(16, experts)
        order = lax.broadcasted_iota(jnp.int32, (count, tokens), 0)
        names = (here + order // local) % groups * local + order % local
        names = jnp.where(order < experts, names, -1)
        tops = routes.shape[0]
        hits = [routes[k : k + 1, :] == names for k in range(tops)]
        picks = sum(jnp.where(hit, 1.0, 0.0) for hit in hits)
        past = lax.broadcasted_iota(jnp.int32, (tokens, tokens), 0)
        present = lax.broadcasted_iota(jnp.int32, (tokens, tokens), 1)
        earlier = mm1(picks, jnp.where(past < present, 1.0, 0.0))
        index = order.astype(f32) * slots + earlier
        row = lax.broadcasted_iota(jnp.int32, (experts * slots, tokens), 0).astype(f32)
        match = [
            row == jnp.sum(jnp.where(hit, index, 0.0), axis=0, keepdims=True) for hit in hits
        ]
        total = sum(scores[k : k + 1, :] for k in range(tops))
        chosen_ref[...] = sum(jnp.where(m, 1.0, 0.0) for m in match).astype(bf16)
        spread = sum(
            jnp.where(match[k], 2.5 * scores[k : k + 1, :] / total, 0.0) for k in range(tops)
        )
        spread_ref[s] = jnp.transpose(spread).astype(bf16)

    def dispatch(s, n, source):
        half = piece // 2
        for i in range(2):
            cols = pl.ds(pl.multiple_of(n * piece + i * half, half), half)
            out = jnp.dot(chosen_ref[...], source[:, cols], preferred_element_type=f32).astype(bf16)
            arrived[s, 0, :, cols] = out[:span]
            leaving[s, 1:, :, cols] = out[span:].reshape(groups - 1, span, half)

        def send(q, carry):
            go_copy(s, q, n).start()
            return carry

        lax.fori_loop(1, groups, send, 0)

    for copy in first_copies:
        copy.wait()
    normalize()
    prepare(0, routes_ref, scores_ref)
    pl.semaphore_wait(barrier, peers + groups - 2)

    for s in range(1, teams):
        for copy in table_copies(s):
            copy.start()
        for n in range(pieces):
            token_copy(s, n).start()
    for s in range(teams):
        slab_copy(s).start()
    for a in range(cuts + 1):
        if a < cuts:
            pair_copy(a).start()
        core_copy(a).start()
        own_copy(a).start()
    for i in range(3):
        shared_copy(i).start()

    def own_piece(n, carry):
        dispatch(0, n, normal)
        return carry

    lax.fori_loop(0, pieces, own_piece, 0)
    for copy in stream_copies:
        copy.wait()
    r_ref, k_ref, v_ref, d_ref, b_ref, gate_ref = (streams.at[i] for i in range(6))

    row = lax.broadcasted_iota(jnp.int32, (two, 2 * two), 0)
    col = lax.broadcasted_iota(jnp.int32, (two, 2 * two), 1)
    state[...] = jnp.where(row == col, 1.0, 0.0)
    turns = r_ref.shape[0] // (BLOCK * unroll)

    def turn(step, carry):
        places = [
            pl.ds(pl.multiple_of((step * unroll + u) * BLOCK, BLOCK), BLOCK) for u in range(unroll)
        ]
        parts = local_blocks(
            [[ref[rows, :] for ref in (r_ref, k_ref, v_ref, d_ref, b_ref)] for rows in places]
        )
        now = state[...]
        for rows, (query_bar, local_out, maps, fade) in zip(places, parts):
            out = mm_scan(query_bar, now)
            qp_ref[rows, :] = out[:, :two]
            lo_ref[rows, :] = out[:, two:] + local_out
            moved = mm_step(maps[:, :two], now) + now * fade
            now = jnp.concatenate([moved[:, :two], moved[:, two:] + maps[:, two:]], axis=1)
        state[...] = now
        return carry

    lax.fori_loop(0, turns, turn, 0)

    carry_map, source_map = state[:, :two], state[:, two:]
    totals[here, 0] = (carry_map[:BLOCK] + carry_map[BLOCK:]).astype(totals.dtype)
    totals[here, 1] = (source_map[:BLOCK] + source_map[BLOCK:]).astype(totals.dtype)

    def ep_copy(q, slot):
        return remote(
            totals.at[slot], totals.at[slot], ep_send.at[q], ep_recv.at[q], column(q)
        )

    for q in range(1, groups):
        ep_copy(q, here).start()

    def widened(s, k):
        for copy in wide_copies(s, k):
            copy.wait_recv()

    def widen(s, k):
        if k:
            widened(s, k - 1)
        else:
            slab_copy(s).wait_recv()
        for copy in wide_copies(s, k):
            copy.start()

    def receive(s, carry):
        for copy in table_copies(s):
            copy.wait_recv()
        prepare(s, other_routes.at[s], other_scores.at[s])

        def other_piece(n, inner):
            token_copy(s, n).wait_recv()
            dispatch(s, n, others.at[s])
            return inner

        return lax.fori_loop(0, pieces, other_piece, carry)

    lax.fori_loop(1, teams, receive, 0)

    for s in range(teams):
        widen(s, 0)

    for i in range(3):
        shared_copy(i).wait()
    step = 256
    for i in range(shared_one.shape[1] // step):
        cols = slice(i * step, (i + 1) * step)
        gate = jnp.dot(normal[...], shared_one[:, cols], preferred_element_type=f32)
        upper = jnp.dot(normal[...], shared_two[:, cols], preferred_element_type=f32)
        shared_hidden[:, cols] = (silu(gate) * upper).astype(bf16)

    def share(i, carry):
        cols = pl.ds(pl.multiple_of(i * step, step), step)
        shared_term[:, cols] = jnp.dot(
            shared_hidden[...], shared_three[:, cols], preferred_element_type=f32
        )
        return carry

    lax.fori_loop(0, width // step, share, 0)

    for q in range(1, groups):
        ep_copy(q, (here + groups - q) % groups).wait_recv()

    def enter(k, entry):
        carry = stacked(totals[k, 0].astype(f32))
        source = stacked(totals[k, 1].astype(f32))
        reached = jnp.where(k < here, 1.0, 0.0)
        return entry + reached * (mm3(carry, entry) + source - entry)

    entry = lax.fori_loop(0, groups, enter, jnp.zeros((two, two), f32))

    def row_copy(q, target, source):
        return remote(
            rows_ref.at[pl.ds(pl.multiple_of(target * tokens, tokens), tokens), :],
            token_ref.at[:, pl.ds(pl.multiple_of(source * two, two), two)],
            row_send.at[q],
            row_recv.at[q],
            {"tp": target},
        )

    def finish(rows):
        recur = mm_fin(qp_ref[rows, :], entry) + lo_ref[rows, :]
        centered = recur - per_head_sum(recur) * (1.0 / HEAD_DIM)
        spread = per_head_sum(centered * centered) * (1.0 / HEAD_DIM)
        normed = centered * lax.rsqrt(spread + 0.00064)
        gated = normed * gain_ref[...] * sigmoid(gate_ref[rows, :].astype(f32))
        rows_ref[rows, :] = gated.astype(bf16)

    def finish_turn(q, carry):
        finish(pl.ds(pl.multiple_of(q * tokens, tokens), tokens))
        return carry

    lax.fori_loop(0, peers, finish_turn, 0)
    nt = (((1,), (1,)), ((), ()))

    def enlarge(s, carry):
        come(s)
        for e in range(local):
            x = arrived[s, :, pl.ds(e * slots, slots), :].reshape(groups * slots, width)
            gate = lax.dot_general(x, weights[2 * e], nt, preferred_element_type=f32)
            upper = lax.dot_general(x, weights[2 * e + 1], nt, preferred_element_type=f32)
            hidden_ref[s, e] = (silu(gate) * upper).astype(bf16)
        return carry

    def reduce(s, n):
        cols = pl.ds(pl.multiple_of(n * piece, piece), piece)
        for e in range(local):
            mine_slots = pl.ds(e * slots, slots)
            out = jnp.dot(hidden_ref[s, e], downs[e, :, cols], preferred_element_type=f32)
            out = out.astype(bf16).reshape(groups, slots, piece)
            returned[s, 0, mine_slots, cols] = out[0]
            arrived[s, 1:, mine_slots, cols] = out[1:]

        def back(q, carry):
            back_copy(s, q, n).start()
            return carry

        lax.fori_loop(1, groups, back, 0)

    def come(s):
        def each(q, carry):
            def some(n, inner):
                go_copy(s, q, n).wait_recv()
                return inner

            return lax.fori_loop(0, pieces, some, carry)

        lax.fori_loop(1, groups, each, 0)

    for a in range(firsts):
        relay(a)
        if a == firsts - 2:
            for k in range(1, bits):
                for s in range(teams):
                    widen(s, k)
    for a in range(firsts):
        own_copy(a).wait()
        ready(a)
    lax.fori_loop(1, teams, enlarge, 0)
    own_rows = pltpu.make_async_copy(
        rows_ref.at[pl.ds(pl.multiple_of(mine * tokens, tokens), tokens), :],
        token_ref.at[:, pl.ds(pl.multiple_of(mine * two, two), two)],
        load_sem.at[cuts + 4],
    )

    def row_start(q, carry):
        row_copy(q, (mine + q) % peers, mine).start()
        return carry

    own_rows.start()
    lax.fori_loop(1, peers, row_start, 0)
    for n in range(pieces):
        a = firsts + n
        relay(a)
        own_copy(a).wait()
        ready(a)

        def mates(s, carry, n=n):
            reduce(s, n)
            return carry

        lax.fori_loop(1, teams, mates, 0)
        if n == pieces // 2:
            for s in range(1, teams):
                widened(s, bits - 1)
                pair_copy(cuts + s).start()
                core_copy(cuts + s).start()

    enlarge(0, 0)

    def mine_too(n, carry):
        reduce(0, n)
        return carry

    lax.fori_loop(0, pieces, mine_too, 0)
    widened(0, bits - 1)
    relay_copy(cuts).start()
    def combined(s, n):
        def each(q, carry):
            back_copy(s, q, n).wait_recv()
            return carry

        lax.fori_loop(1, groups, each, 0)
        cols = pl.ds(pl.multiple_of(n * piece, piece), piece)
        rows = returned[s, :, :, cols].reshape(groups * span, piece)
        return jnp.dot(spread_ref[s], rows, preferred_element_type=f32), cols

    def partial(s, carry):
        def some(n, inner):
            value, cols = combined(s, n)
            part_out[s, :, cols] = value.astype(bf16)
            part_copy(s, n).start()
            return inner

        return lax.fori_loop(0, pieces, some, carry)

    lax.fori_loop(1, teams, partial, 0)

    for a in range(cuts + 1, cuts + teams):
        relay(a)
    own_copy(cuts).wait()
    for a in range(cuts, cuts + teams):
        ready(a)
    own_rows.wait()

    def row_end(q, carry):
        row_copy(q, (mine + q) % peers, (mine + peers - q) % peers).wait()
        return carry

    lax.fori_loop(1, peers, row_end, 0)

    def mix(i, carry):
        cols = pl.ds(pl.multiple_of(i * step, step), step)
        mixed_ref[:, cols] = jnp.dot(
            token_ref[...], project[:, cols], preferred_element_type=f32
        ).astype(bf16)
        return carry

    lax.fori_loop(0, width // step, mix, 0)

    def close(n, carry):
        value, cols = combined(0, n)
        total = value + shared_term[:, cols]
        for s in range(1, teams):
            part_copy(s, n).wait_recv()
            total = total + part_in[s, :, cols].astype(f32)
        moe_ref[:, cols] = total.astype(bf16)
        return carry

    lax.fori_loop(0, pieces, close, 0)

    for a in range(cuts + teams):
        if a != cuts:
            pair_copy(a).wait_send()
        core_copy(a).wait_send()
        relay_copy(a).wait_send()
    for q in range(1, groups):
        ep_copy(q, here).wait_send()

    def sent(s, carry):
        def each(q, inner):
            def block(n, last):
                go_copy(s, q, n).wait_send()
                back_copy(s, q, n).wait_send()
                return last

            return lax.fori_loop(0, pieces, block, inner)

        return lax.fori_loop(1, groups, each, carry)

    lax.fori_loop(0, teams, sent, 0)

    def shipped(s, carry):
        for copy in table_copies(s):
            copy.wait_send()

        def block(n, inner):
            part_copy(s, n).wait_send()
            token_copy(s, n).wait_send()
            return inner

        return lax.fori_loop(0, pieces, block, carry)

    lax.fori_loop(1, teams, shipped, 0)
    for s in range(teams):
        slab_copy(s).wait_send()
        for k in range(bits):
            for copy in wide_copies(s, k):
                copy.wait_send()


def shards(
    receptance,
    key_in,
    payload_vectors,
    decay_in,
    rate_in,
    gate_in,
    norm_gain,
    out_weight,
    moe_in,
    moe_gain,
    routes,
    route_weights,
    expert_gate,
    expert_up,
    expert_down,
    shared_gate,
    shared_up,
    shared_down,
):
    length, channels = receptance.shape
    tokens, width = moe_in.shape
    groups, peers = lax.axis_size("ep"), lax.axis_size("tp")
    teams = peers // 4
    local, _, height = expert_gate.shape
    top_count = routes.shape[1]
    experts = local * groups
    slots = max(2, 3 * tokens * top_count // (2 * experts))
    slots = -(-slots // 16) * 16
    span = local * slots
    inner = shared_gate.shape[1]
    pieces = 4
    cuts = 2 * local + pieces
    wide = 2 * HEAD_DIM
    spare = wide - channels
    pad = lambda x: jnp.pad(x, ((0, 0),) * (x.ndim - 1) + ((0, spare),)) if spare else x
    weight_rows = jnp.pad(out_weight, ((0, spare), (0, 0))) if spare else out_weight
    f32, bf16 = jnp.float32, jnp.bfloat16
    vmem = pl.BlockSpec(memory_space=pltpu.VMEM)
    anywhere = pl.BlockSpec(memory_space=pl.ANY)
    dma = pltpu.SemaphoreType.DMA
    out = pltpu.VMEM((tokens, width), bf16)
    turned = lambda w: jnp.swapaxes(w, 1, 2)
    return pl.pallas_call(
        functools.partial(layer_kernel, 8, pieces, slots),
        out_shape=(out, out),
        in_specs=[anywhere] * 18,
        out_specs=(vmem, vmem),
        scratch_shapes=[
            pltpu.VMEM((tokens, width), bf16),
            pltpu.VMEM((1, width), f32),
            pltpu.VMEM((top_count, tokens), jnp.int32),
            pltpu.VMEM((top_count, tokens), f32),
            pltpu.VMEM((1, wide), f32),
            pltpu.VMEM((6, length, wide), bf16),
            pltpu.VMEM((wide, 2 * wide), f32),
            pltpu.VMEM((length, wide), f32),
            pltpu.VMEM((length, wide), f32),
            pltpu.VMEM((length, wide), bf16),
            pltpu.VMEM((groups, 2, HEAD_DIM, wide), bf16),
            pltpu.VMEM((tokens, peers * wide), bf16),
            pltpu.VMEM((peers * wide, width), bf16),
            pltpu.VMEM((2 * local, 4 * height, width), bf16),
            pltpu.VMEM((local, 4 * height, width), bf16),
            pltpu.VMEM(shared_gate.shape, bf16),
            pltpu.VMEM(shared_up.shape, bf16),
            pltpu.VMEM(shared_down.shape, bf16),
            pltpu.VMEM((tokens, inner), bf16),
            pltpu.VMEM((tokens, width), f32),
            pltpu.VMEM((teams, tokens, width), bf16),
            pltpu.VMEM((teams, top_count, tokens), jnp.int32),
            pltpu.VMEM((teams, top_count, tokens), f32),
            pltpu.VMEM((tokens, width), bf16),
            pltpu.VMEM((experts * slots, tokens), bf16),
            pltpu.VMEM((teams, tokens, experts * slots), bf16),
            pltpu.VMEM((teams, groups, span, width), bf16),
            pltpu.VMEM((teams, groups, span, width), bf16),
            pltpu.VMEM((teams, groups, span, width), bf16),
            pltpu.VMEM((teams, local, groups * slots, 4 * height), bf16),
            pltpu.VMEM((teams, tokens, width), bf16),
            pltpu.VMEM((teams, tokens, width), bf16),
            dma((teams, 2)),
            dma((teams, 2)),
            dma((teams, pieces)),
            dma((teams, pieces)),
            dma((teams,)),
            dma((teams,)),
            dma((teams, groups)),
            dma((teams, groups)),
            dma((cuts + teams,)),
            dma((cuts + teams,)),
            dma((cuts + teams,)),
            dma((cuts + teams,)),
            dma((cuts + teams,)),
            dma((cuts + teams,)),
            dma((cuts + 5,)),
            dma((11,)),
            dma((teams, groups, pieces)),
            dma((teams, groups, pieces)),
            dma((teams, groups, pieces)),
            dma((teams, groups, pieces)),
            dma((teams, pieces)),
            dma((teams, pieces)),
            dma((groups,)),
            dma((groups,)),
            dma((peers,)),
            dma((peers,)),
        ],
        compiler_params=pltpu.CompilerParams(
            collective_id=0, has_side_effects=True, vmem_limit_bytes=62 << 20
        ),
    )(
        pad(norm_gain).reshape(1, wide),
        moe_in,
        moe_gain.reshape(1, width),
        routes.T,
        route_weights.T,
        pad(receptance),
        pad(key_in),
        pad(payload_vectors),
        pad(decay_in),
        pad(rate_in),
        pad(gate_in),
        weight_rows,
        turned(expert_gate),
        turned(expert_up),
        turned(expert_down),
        shared_gate,
        shared_up,
        shared_down,
    )


def solution(mesh):
    placed = (
        P("ep", "tp"),
        P("ep", "tp"),
        P("ep", "tp"),
        P("ep", "tp"),
        P("ep", "tp"),
        P("ep", "tp"),
        P("tp"),
        P("tp", None),
        P(("ep", "tp"), None),
        P(),
        P(("ep", "tp"), None),
        P(("ep", "tp"), None),
        P("ep", None, "tp"),
        P("ep", None, "tp"),
        P("ep", None, "tp"),
        P(),
        P(),
        P(),
    )
    return jax.shard_map(
        shards,
        mesh=mesh,
        in_specs=placed,
        out_specs=(P(("ep", "tp"), None), P(("ep", "tp"), None)),
        check_vma=False,
    )
```

```python
import functools

import jax
import jax.numpy as jnp
from jax import lax
from jax.experimental import pallas as pl
from jax.experimental.pallas import tpu as pltpu
from jax.sharding import PartitionSpec as P

HEAD_DIM = 64
BLOCK = 64


def dims(form):
    return {"nn": ((1,), (0,)), "nt": ((1,), (1,)), "tn": ((0,), (0,))}[form]


def mm1(left, right, form="nn"):
    return lax.dot_general(
        left.astype(jnp.bfloat16),
        right.astype(jnp.bfloat16),
        (dims(form), ((), ())),
        preferred_element_type=jnp.float32,
    )


def mm3(left, right, form="nn"):
    lh, rh = left.astype(jnp.bfloat16), right.astype(jnp.bfloat16)
    ll = (left - lh.astype(jnp.float32)).astype(jnp.bfloat16)
    rl = (right - rh.astype(jnp.float32)).astype(jnp.bfloat16)
    return mm1(lh, rh, form) + (mm1(lh, rl, form) + mm1(ll, rh, form))


mm_g = mm1
mm_inv = mm1
mm_q = mm1
mm_out = mm1
mm_car = mm1
mm_scan = mm1
mm_step = mm1
mm_fin = mm1


def head_masks(rows, width):
    lane = lax.broadcasted_iota(jnp.int32, (rows, width), 1)
    return lane < HEAD_DIM


def stacked(x):
    first = head_masks(*x.shape)
    return jnp.concatenate([jnp.where(first, x, 0.0), jnp.where(first, 0.0, x)], axis=0)


def per_head_sum(x):
    first = head_masks(*x.shape)
    one = jnp.sum(jnp.where(first, x, 0.0), axis=-1, keepdims=True)
    both = jnp.sum(jnp.where(first, 0.0, x), axis=-1, keepdims=True)
    return jnp.where(first, one, both)


def sigmoid(x):
    return 1.0 / (1.0 + jnp.exp(-x))


def block_stages(r_in, k_in, v_in, d_in, b_in):
    f32 = jnp.float32
    keys = k_in.astype(f32)
    unit = keys * lax.rsqrt(per_head_sum(keys * keys) + 1e-06)
    log_decay = sigmoid(d_in.astype(f32)) * -0.6065306597126334
    tri_row = lax.broadcasted_iota(jnp.int32, (BLOCK, 3 * BLOCK), 0)
    tri_col = lax.broadcasted_iota(jnp.int32, (BLOCK, 3 * BLOCK), 1) % BLOCK
    tri = jnp.where(tri_col <= tri_row, 1.0, 0.0).astype(jnp.bfloat16)
    hi = log_decay.astype(jnp.bfloat16)
    rest = log_decay - hi.astype(f32)
    mid = rest.astype(jnp.bfloat16)
    low = (rest - mid.astype(f32)).astype(jnp.bfloat16)
    cumul = mm1(tri, jnp.concatenate([hi, mid, low], axis=0))
    yield
    end_scale = jnp.exp(cumul[BLOCK - 1 :, :])
    shrink = jnp.exp(-cumul)
    query = r_in.astype(f32) * jnp.exp(cumul)
    alpha = -unit * jnp.exp(cumul - log_decay)
    key_grow = keys * shrink
    beta_grow = unit * sigmoid(b_in.astype(f32)) * shrink
    values = v_in.astype(f32)
    values2 = stacked(values)
    two = 2 * BLOCK
    grams = mm_g(
        jnp.concatenate([alpha, query], axis=0),
        jnp.concatenate([stacked(beta_grow), stacked(key_grow)], axis=0),
        "nt",
    )
    yield
    row = lax.broadcasted_iota(jnp.int32, (BLOCK, two), 0)
    col = lax.broadcasted_iota(jnp.int32, (BLOCK, two), 1) % BLOCK
    strict = col < row
    inclusive = col <= row
    couple = jnp.where(strict, grams[:BLOCK, :two], 0.0)
    insert = jnp.where(strict, grams[:BLOCK, two:], 0.0)
    read_beta = jnp.where(inclusive, grams[BLOCK:, :two], 0.0)
    read_key = jnp.where(inclusive, grams[BLOCK:, two:], 0.0)
    size = 8
    near = jnp.where(row // size == col // size, couple, 0.0)
    inverse = jnp.where(row == col, 1.0, 0.0) + near
    power = mm_inv(near, stacked(near))
    yield
    both = mm_inv(jnp.concatenate([inverse, power], axis=0), stacked(power))
    yield
    inverse = inverse + both[:BLOCK]
    inverse = inverse + mm_inv(inverse, stacked(both[BLOCK:]))
    yield
    while size < BLOCK:
        wide = 2 * size
        off = jnp.where(
            (row // wide == col // wide) & (row // size != col // size), couple, 0.0
        )
        step = mm_inv(off, stacked(inverse))
        yield
        inverse = inverse + mm_inv(inverse, stacked(step))
        yield
        size = wide
    inserted = mm_q(insert, values2)
    yield
    qz = mm_q(inverse, jnp.concatenate([stacked(alpha), stacked(inserted)], axis=1))
    yield
    q_rows, z_rows = qz[:, :two], qz[:, two:]
    upper = jnp.concatenate([stacked(q_rows), stacked(z_rows)], axis=1)
    lower = jnp.concatenate([jnp.zeros_like(values2), values2], axis=1)
    reads = mm_out(
        jnp.concatenate([read_beta, read_key], axis=1), jnp.concatenate([upper, lower], axis=0)
    )
    yield
    query_bar = query + reads[:, :two]
    local_out = reads[:, two:]
    ends = jnp.concatenate([beta_grow * end_scale, key_grow * end_scale], axis=0)
    lower = jnp.concatenate([jnp.zeros_like(values), values], axis=1)
    maps = mm_car(ends, jnp.concatenate([qz, lower], axis=0), "tn")
    yield
    head_row = lax.broadcasted_iota(jnp.int32, (two, 2 * two), 0) // HEAD_DIM
    head_col = lax.broadcasted_iota(jnp.int32, (two, 2 * two), 1) % two // HEAD_DIM
    maps = jnp.where(head_row == head_col, maps, 0.0)
    row = lax.broadcasted_iota(jnp.int32, (two, two), 0)
    col = lax.broadcasted_iota(jnp.int32, (two, two), 1)
    fade = jnp.sum(jnp.where(row == col, end_scale, 0.0), axis=1, keepdims=True)
    return query_bar, local_out, maps, fade


def local_blocks(inputs):
    stages = [block_stages(*block) for block in inputs]
    results = [None] * len(stages)
    while None in results:
        for i, stage in enumerate(stages):
            try:
                next(stage)
            except StopIteration as end:
                results[i] = end.value
    return results


def silu(x):
    return x / (1.0 + jnp.exp(-x))


def layer_kernel(
    unroll,
    pieces,
    slots,
    gain_in,
    x_in,
    moe_gain_in,
    routes_in,
    scores_in,
    r_in,
    k_in,
    v_in,
    d_in,
    b_in,
    gate_in,
    project_in,
    expert_gate,
    expert_up,
    expert_down,
    shared_gate,
    shared_up,
    shared_down,
    mixed_ref,
    moe_ref,
    x_ref,
    moe_gain_ref,
    routes_ref,
    scores_ref,
    gain_ref,
    streams,
    state,
    qp_ref,
    lo_ref,
    rows_ref,
    totals,
    token_ref,
    project,
    weights,
    downs,
    shared_one,
    shared_two,
    shared_three,
    shared_hidden,
    shared_term,
    others,
    other_routes,
    other_scores,
    normal,
    chosen_ref,
    spread_ref,
    leaving,
    arrived,
    returned,
    hidden_ref,
    part_out,
    part_in,
    table_send,
    table_recv,
    token_send,
    token_recv,
    slab_send,
    slab_recv,
    wide_send,
    wide_recv,
    pair_send,
    pair_recv,
    core_send,
    core_recv,
    relay_send,
    relay_recv,
    load_sem,
    stream_sem,
    go_send,
    go_recv,
    back_send,
    back_recv,
    part_send,
    part_recv,
    ep_send,
    ep_recv,
    row_send,
    row_recv,
):
    f32, bf16 = jnp.float32, jnp.bfloat16
    two = 2 * BLOCK
    MESH = pl.DeviceIdType.MESH
    first_pairs = (
        (x_in, x_ref),
        (moe_gain_in, moe_gain_ref),
        (routes_in, routes_ref),
        (scores_in, scores_ref),
        (gain_in, gain_ref),
    )
    first_copies = [
        pltpu.make_async_copy(source, target, stream_sem.at[6 + i])
        for i, (source, target) in enumerate(first_pairs)
    ]
    stream_copies = [
        pltpu.make_async_copy(source, streams.at[i], stream_sem.at[i])
        for i, source in enumerate((r_in, k_in, v_in, d_in, b_in, gate_in))
    ]
    for copy in first_copies + stream_copies:
        copy.start()
    here, mine = lax.axis_index("ep"), lax.axis_index("tp")
    groups, peers = lax.axis_size("ep"), lax.axis_size("tp")
    depth, core = mine // 2, mine % 2
    teams = peers // 4
    team, side = depth // 2, depth % 2
    seat = side * 2 + core
    facing = (1 - side) * 2 + core
    partner = depth * 2 + 1 - core
    across = team * 4 + facing
    tokens, width = x_in.shape
    local, height = expert_gate.shape[0], expert_gate.shape[1]
    experts = local * groups
    span = local * slots
    columns = width // groups
    piece = width // pieces
    sources = (expert_gate, expert_up)
    firsts = 2 * local
    cuts = firsts + pieces

    def remote(source, target, send, recv, device):
        return pltpu.make_async_remote_copy(
            src_ref=source,
            dst_ref=target,
            send_sem=send,
            recv_sem=recv,
            device_id=device,
            device_id_type=MESH,
        )

    def mate(shift):
        return {"tp": (team + shift) % teams * 4 + seat}

    def column(shift):
        return {"ep": (here + groups + shift) % groups}

    def table_copies(s):
        pairs = ((routes_ref, other_routes), (scores_ref, other_scores))
        return [
            remote(a, b.at[s], table_send.at[s, i], table_recv.at[s, i], mate(s))
            for i, (a, b) in enumerate(pairs)
        ]

    def token_copy(s, n):
        cols = pl.ds(pl.multiple_of(n * piece, piece), piece)
        return remote(
            normal.at[:, cols],
            others.at[s, :, cols],
            token_send.at[s, n],
            token_recv.at[s, n],
            mate(s),
        )

    def slab_place(owner, part):
        return project.at[
            pl.ds(pl.multiple_of(owner * two, two), two),
            pl.ds(pl.multiple_of(part * columns, columns), columns),
        ]

    def slab_copy(s):
        source = project_in.at[:, pl.ds(pl.multiple_of(here * columns, columns), columns)]
        target = mate(s) if s else {"tp": across}
        return remote(source, slab_place(mine, here), slab_send.at[s], slab_recv.at[s], target)

    bits = groups.bit_length() - 1

    def flipped(mask):
        place = here
        for i in range(bits):
            if mask >> i & 1:
                place = place + (1 << i) * (1 - here // (1 << i) % 2 * 2)
        return place

    def wide_copy(s, k, j):
        owner = (team + teams - s) % teams * 4 + seat if s else across
        order = [(i + s) % bits for i in range(bits)]
        mask = sum((j >> i & 1) << order[i] for i in range(k))
        block = slab_place(owner, flipped(mask))
        slot = (1 << k) + j
        target = {"ep": flipped(1 << order[k])}
        return remote(block, block, wide_send.at[s, slot], wide_recv.at[s, slot], target)

    def wide_copies(s, k):
        return [wide_copy(s, k, j) for j in range(1 << k)]

    def weight_place(a, owner):
        rows = pl.ds(pl.multiple_of(owner * height, height), height)
        if a < firsts:
            return weights.at[a, rows, :]
        return downs.at[:, rows, pl.ds((a - firsts) * piece, piece)]

    def project_place(s, owner):
        base = (team + teams - s) % teams * 4 + owner
        return project.at[pl.ds(pl.multiple_of(base * two, two), two), :]

    def place_of(a, owner):
        return weight_place(a, owner) if a < cuts else project_place(a - cuts, owner)

    def own_block(a):
        if a < firsts:
            return sources[a % 2].at[a // 2]
        if a < cuts:
            return expert_down.at[:, :, pl.ds((a - firsts) * piece, piece)]
        return project_in if a == cuts else project_place(a - cuts, seat)

    def pair_copy(a):
        return remote(
            own_block(a), place_of(a, seat), pair_send.at[a], pair_recv.at[a], {"tp": across}
        )

    def core_copy(a):
        return remote(
            own_block(a), place_of(a, seat), core_send.at[a], core_recv.at[a], {"tp": partner}
        )

    def relay_copy(a):
        block = place_of(a, facing)
        return remote(block, block, relay_send.at[a], relay_recv.at[a], {"tp": partner})

    def own_copy(a):
        return pltpu.make_async_copy(own_block(a), place_of(a, seat), load_sem.at[a])

    def relay(a):
        pair_copy(a).wait_recv()
        relay_copy(a).start()

    def ready(a):
        core_copy(a).wait_recv()
        relay_copy(a).wait_recv()

    def shared_copy(i):
        source = (shared_gate, shared_up, shared_down)[i]
        target = (shared_one, shared_two, shared_three)[i]
        return pltpu.make_async_copy(source, target, load_sem.at[cuts + 1 + i])

    def go_copy(s, q, n):
        cols = pl.ds(pl.multiple_of(n * piece, piece), piece)
        return remote(
            leaving.at[s, q, :, cols],
            arrived.at[s, q, :, cols],
            go_send.at[s],
            go_recv.at[s],
            column(q),
        )

    def back_copy(s, q, n):
        cols = pl.ds(pl.multiple_of(n * piece, piece), piece)
        return remote(
            arrived.at[s, q, :, cols],
            returned.at[s, q, :, cols],
            back_send.at[s],
            back_recv.at[s, n],
            column(-q),
        )

    others_of = pl.ds(1, groups - 1)

    def go_all(s):
        return remote(
            leaving.at[s, others_of], arrived.at[s, others_of], go_send.at[s], go_recv.at[s], column(1)
        )

    def back_all(s):
        return remote(
            arrived.at[s, others_of],
            returned.at[s, others_of],
            back_send.at[s],
            back_recv.at[s, 0],
            column(1),
        )

    def back_piece(s, n):
        cols = pl.ds(pl.multiple_of(n * piece, piece), piece)
        return remote(
            arrived.at[s, others_of, :, cols],
            returned.at[s, others_of, :, cols],
            back_send.at[s],
            back_recv.at[s, n],
            column(1),
        )

    def part_copy(s, n):
        cols = pl.ds(pl.multiple_of(n * piece, piece), piece)
        return remote(
            part_out.at[s, :, cols],
            part_in.at[s, :, cols],
            part_send.at[s, n],
            part_recv.at[s, n],
            mate(teams - s),
        )

    barrier = pltpu.get_barrier_semaphore()
    for q in range(1, peers):
        pl.semaphore_signal(
            barrier, inc=1, device_id={"tp": (mine + q) % peers}, device_id_type=MESH
        )
    for q in range(1, groups):
        pl.semaphore_signal(
            barrier, inc=1, device_id={"ep": (here + q) % groups}, device_id_type=MESH
        )
    def normalize():
        tall = 16

        def some(i, carry):
            rows = pl.ds(pl.multiple_of(i * tall, tall), tall)
            values = x_ref[rows, :].astype(f32)
            centered = values - jnp.sum(values, -1, keepdims=True) * (1.0 / width)
            spread = jnp.sum(centered * centered, -1, keepdims=True) * (1.0 / width)
            normal[rows, :] = (centered * lax.rsqrt(spread + 1e-05) * moe_gain_ref[...]).astype(
                bf16
            )
            return carry

        lax.fori_loop(0, tokens // tall, some, 0)

    def prepare(s, routes, scores):
        count = max(16, experts)
        order = lax.broadcasted_iota(jnp.int32, (count, tokens), 0)
        names = (here + order // local) % groups * local + order % local
        names = jnp.where(order < experts, names, -1)
        tops = routes.shape[0]
        hits = [routes[k : k + 1, :] == names for k in range(tops)]
        picks = sum(jnp.where(hit, 1.0, 0.0) for hit in hits)
        past = lax.broadcasted_iota(jnp.int32, (tokens, tokens), 0)
        present = lax.broadcasted_iota(jnp.int32, (tokens, tokens), 1)
        earlier = mm1(picks, jnp.where(past < present, 1.0, 0.0))
        index = order.astype(f32) * slots + earlier
        row = lax.broadcasted_iota(jnp.int32, (experts * slots, tokens), 0).astype(f32)
        match = [
            row == jnp.sum(jnp.where(hit, index, 0.0), axis=0, keepdims=True) for hit in hits
        ]
        total = sum(scores[k : k + 1, :] for k in range(tops))
        chosen_ref[...] = sum(jnp.where(m, 1.0, 0.0) for m in match).astype(bf16)
        spread = sum(
            jnp.where(match[k], 2.5 * scores[k : k + 1, :] / total, 0.0) for k in range(tops)
        )
        spread_ref[s] = jnp.transpose(spread).astype(bf16)

    def dispatch(s, n, source):
        half = piece // 2
        for i in range(2):
            cols = pl.ds(pl.multiple_of(n * piece + i * half, half), half)
            out = jnp.dot(chosen_ref[...], source[:, cols], preferred_element_type=f32).astype(bf16)
            arrived[s, 0, :, cols] = out[:span]
            leaving[s, 1:, :, cols] = out[span:].reshape(groups - 1, span, half)

        def send(q, carry):
            go_copy(s, q, n).start()
            return carry

        lax.fori_loop(1, groups, send, 0)

    for copy in first_copies:
        copy.wait()
    normalize()
    prepare(0, routes_ref, scores_ref)
    pl.semaphore_wait(barrier, peers + groups - 2)

    for s in range(1, teams):
        for copy in table_copies(s):
            copy.start()
    early = 1
    for a in range(early):
        pair_copy(a).start()
    for s in range(1, teams):
        for n in range(pieces):
            token_copy(s, n).start()
    for s in range(teams):
        slab_copy(s).start()
    for a in range(cuts + 1):
        if early <= a < cuts:
            pair_copy(a).start()
        core_copy(a).start()
        own_copy(a).start()
    for i in range(3):
        shared_copy(i).start()

    def own_piece(n, carry):
        dispatch(0, n, normal)
        return carry

    lax.fori_loop(0, pieces, own_piece, 0)
    for copy in stream_copies:
        copy.wait()
    r_ref, k_ref, v_ref, d_ref, b_ref, gate_ref = (streams.at[i] for i in range(6))

    row = lax.broadcasted_iota(jnp.int32, (two, 2 * two), 0)
    col = lax.broadcasted_iota(jnp.int32, (two, 2 * two), 1)
    state[...] = jnp.where(row == col, 1.0, 0.0)
    turns = r_ref.shape[0] // (BLOCK * unroll)

    def turn(step, carry):
        places = [
            pl.ds(pl.multiple_of((step * unroll + u) * BLOCK, BLOCK), BLOCK) for u in range(unroll)
        ]
        parts = local_blocks(
            [[ref[rows, :] for ref in (r_ref, k_ref, v_ref, d_ref, b_ref)] for rows in places]
        )
        now = state[...]
        for rows, (query_bar, local_out, maps, fade) in zip(places, parts):
            out = mm_scan(query_bar, now)
            qp_ref[rows, :] = out[:, :two]
            lo_ref[rows, :] = out[:, two:] + local_out
            moved = mm_step(maps[:, :two], now) + now * fade
            now = jnp.concatenate([moved[:, :two], moved[:, two:] + maps[:, two:]], axis=1)
        state[...] = now
        return carry

    lax.fori_loop(0, turns, turn, 0)

    carry_map, source_map = state[:, :two], state[:, two:]
    totals[here, 0] = (carry_map[:BLOCK] + carry_map[BLOCK:]).astype(totals.dtype)
    totals[here, 1] = (source_map[:BLOCK] + source_map[BLOCK:]).astype(totals.dtype)

    def ep_copy(q, slot):
        return remote(
            totals.at[slot], totals.at[slot], ep_send.at[q], ep_recv.at[q], column(q)
        )

    for q in range(1, groups):
        ep_copy(q, here).start()

    def widened(s, k):
        for copy in wide_copies(s, k):
            copy.wait_recv()

    def widen(s, k):
        if k:
            widened(s, k - 1)
        else:
            slab_copy(s).wait_recv()
        for copy in wide_copies(s, k):
            copy.start()

    def receive(s, carry):
        for copy in table_copies(s):
            copy.wait_recv()
        prepare(s, other_routes.at[s], other_scores.at[s])

        def other_piece(n, inner):
            token_copy(s, n).wait_recv()
            dispatch(s, n, others.at[s])
            return inner

        return lax.fori_loop(0, pieces, other_piece, carry)

    lax.fori_loop(1, teams, receive, 0)

    for s in range(teams):
        widen(s, 0)

    for i in range(3):
        shared_copy(i).wait()
    step = 256
    for i in range(shared_one.shape[1] // step):
        cols = slice(i * step, (i + 1) * step)
        gate = jnp.dot(normal[...], shared_one[:, cols], preferred_element_type=f32)
        upper = jnp.dot(normal[...], shared_two[:, cols], preferred_element_type=f32)
        shared_hidden[:, cols] = (silu(gate) * upper).astype(bf16)

    def share(i, carry):
        cols = pl.ds(pl.multiple_of(i * step, step), step)
        shared_term[:, cols] = jnp.dot(
            shared_hidden[...], shared_three[:, cols], preferred_element_type=f32
        )
        return carry

    lax.fori_loop(0, width // step, share, 0)

    for q in range(1, groups):
        ep_copy(q, (here + groups - q) % groups).wait_recv()

    def enter(k, entry):
        carry = stacked(totals[k, 0].astype(f32))
        source = stacked(totals[k, 1].astype(f32))
        reached = jnp.where(k < here, 1.0, 0.0)
        return entry + reached * (mm3(carry, entry) + source - entry)

    entry = lax.fori_loop(0, groups, enter, jnp.zeros((two, two), f32))

    def row_copy(q, target, source):
        return remote(
            rows_ref.at[pl.ds(pl.multiple_of(target * tokens, tokens), tokens), :],
            token_ref.at[:, pl.ds(pl.multiple_of(source * two, two), two)],
            row_send.at[q],
            row_recv.at[q],
            {"tp": target},
        )

    def finish(rows):
        recur = mm_fin(qp_ref[rows, :], entry) + lo_ref[rows, :]
        centered = recur - per_head_sum(recur) * (1.0 / HEAD_DIM)
        spread = per_head_sum(centered * centered) * (1.0 / HEAD_DIM)
        normed = centered * lax.rsqrt(spread + 0.00064)
        gated = normed * gain_ref[...] * sigmoid(gate_ref[rows, :].astype(f32))
        rows_ref[rows, :] = gated.astype(bf16)

    def finish_turn(q, carry):
        finish(pl.ds(pl.multiple_of(q * tokens, tokens), tokens))
        return carry

    lax.fori_loop(0, peers, finish_turn, 0)
    nt = (((1,), (1,)), ((), ()))

    def enlarge(s, carry):
        come(s)
        for e in range(local):
            x = arrived[s, :, pl.ds(e * slots, slots), :].reshape(groups * slots, width)
            gate = lax.dot_general(x, weights[2 * e], nt, preferred_element_type=f32)
            upper = lax.dot_general(x, weights[2 * e + 1], nt, preferred_element_type=f32)
            hidden_ref[s, e] = (silu(gate) * upper).astype(bf16)
        return carry

    def reduce(s, n):
        cols = pl.ds(pl.multiple_of(n * piece, piece), piece)
        for e in range(local):
            mine_slots = pl.ds(e * slots, slots)
            out = jnp.dot(hidden_ref[s, e], downs[e, :, cols], preferred_element_type=f32)
            out = out.astype(bf16).reshape(groups, slots, piece)
            returned[s, 0, mine_slots, cols] = out[0]
            arrived[s, 1:, mine_slots, cols] = out[1:]

        def back(q, carry):
            back_copy(s, q, n).start()
            return carry

        lax.fori_loop(1, groups, back, 0)

    def come(s):
        go_all(s).wait_recv()

    for a in range(firsts):
        relay(a)
        if a == firsts - 2:
            for k in range(1, bits):
                for s in range(teams):
                    widen(s, k)
    for a in range(firsts):
        own_copy(a).wait()
        ready(a)
    lax.fori_loop(1, teams, enlarge, 0)
    own_rows = pltpu.make_async_copy(
        rows_ref.at[pl.ds(pl.multiple_of(mine * tokens, tokens), tokens), :],
        token_ref.at[:, pl.ds(pl.multiple_of(mine * two, two), two)],
        load_sem.at[cuts + 4],
    )

    def row_start(q, carry):
        row_copy(q, (mine + q) % peers, mine).start()
        return carry

    own_rows.start()
    lax.fori_loop(1, peers, row_start, 0)
    for n in range(pieces):
        a = firsts + n
        relay(a)
        own_copy(a).wait()
        ready(a)

        def mates(s, carry, n=n):
            reduce(s, n)
            return carry

        lax.fori_loop(1, teams, mates, 0)
        if n == 0:
            enlarge(0, 0)
        if n == pieces // 2:
            for s in range(1, teams):
                widened(s, bits - 1)
                pair_copy(cuts + s).start()
                core_copy(cuts + s).start()

    def mine_too(n, carry):
        reduce(0, n)
        return carry

    lax.fori_loop(0, pieces, mine_too, 0)
    widened(0, bits - 1)
    relay_copy(cuts).start()
    def combined(s, n):
        back_piece(s, n).wait_recv()
        cols = pl.ds(pl.multiple_of(n * piece, piece), piece)
        rows = returned[s, :, :, cols].reshape(groups * span, piece)
        return jnp.dot(spread_ref[s], rows, preferred_element_type=f32), cols

    def partial(s, carry):
        def some(n, inner):
            value, cols = combined(s, n)
            part_out[s, :, cols] = value.astype(bf16)
            part_copy(s, n).start()
            return inner

        return lax.fori_loop(0, pieces, some, carry)

    lax.fori_loop(1, teams, partial, 0)

    for a in range(cuts + 1, cuts + teams):
        relay(a)
    own_copy(cuts).wait()
    for a in range(cuts, cuts + teams):
        ready(a)
    own_rows.wait()

    def row_end(q, carry):
        row_copy(q, (mine + q) % peers, (mine + peers - q) % peers).wait()
        return carry

    lax.fori_loop(1, peers, row_end, 0)

    def mix(i, carry):
        cols = pl.ds(pl.multiple_of(i * step, step), step)
        mixed_ref[:, cols] = jnp.dot(
            token_ref[...], project[:, cols], preferred_element_type=f32
        ).astype(bf16)
        return carry

    lax.fori_loop(0, width // step, mix, 0)

    def close(n, carry):
        value, cols = combined(0, n)
        total = value + shared_term[:, cols]
        for s in range(1, teams):
            part_copy(s, n).wait_recv()
            total = total + part_in[s, :, cols].astype(f32)
        moe_ref[:, cols] = total.astype(bf16)
        return carry

    lax.fori_loop(0, pieces, close, 0)

    for a in range(cuts + teams):
        if a != cuts:
            pair_copy(a).wait_send()
        core_copy(a).wait_send()
        relay_copy(a).wait_send()
    for q in range(1, groups):
        ep_copy(q, here).wait_send()

    def sent(s, carry):
        go_all(s).wait_send()
        back_all(s).wait_send()
        return carry

    lax.fori_loop(0, teams, sent, 0)

    def shipped(s, carry):
        for copy in table_copies(s):
            copy.wait_send()

        def block(n, inner):
            part_copy(s, n).wait_send()
            token_copy(s, n).wait_send()
            return inner

        return lax.fori_loop(0, pieces, block, carry)

    lax.fori_loop(1, teams, shipped, 0)
    for s in range(teams):
        slab_copy(s).wait_send()
        for k in range(bits):
            for copy in wide_copies(s, k):
                copy.wait_send()


def shards(
    receptance,
    key_in,
    payload_vectors,
    decay_in,
    rate_in,
    gate_in,
    norm_gain,
    out_weight,
    moe_in,
    moe_gain,
    routes,
    route_weights,
    expert_gate,
    expert_up,
    expert_down,
    shared_gate,
    shared_up,
    shared_down,
):
    length, channels = receptance.shape
    tokens, width = moe_in.shape
    groups, peers = lax.axis_size("ep"), lax.axis_size("tp")
    teams = peers // 4
    local, _, height = expert_gate.shape
    top_count = routes.shape[1]
    experts = local * groups
    slots = max(2, 3 * tokens * top_count // (2 * experts))
    slots = -(-slots // 16) * 16
    span = local * slots
    inner = shared_gate.shape[1]
    pieces = 4
    cuts = 2 * local + pieces
    wide = 2 * HEAD_DIM
    spare = wide - channels
    pad = lambda x: jnp.pad(x, ((0, 0),) * (x.ndim - 1) + ((0, spare),)) if spare else x
    weight_rows = jnp.pad(out_weight, ((0, spare), (0, 0))) if spare else out_weight
    f32, bf16 = jnp.float32, jnp.bfloat16
    vmem = pl.BlockSpec(memory_space=pltpu.VMEM)
    anywhere = pl.BlockSpec(memory_space=pl.ANY)
    dma = pltpu.SemaphoreType.DMA
    out = pltpu.VMEM((tokens, width), bf16)
    turned = lambda w: jnp.swapaxes(w, 1, 2)
    return pl.pallas_call(
        functools.partial(layer_kernel, 8, pieces, slots),
        out_shape=(out, out),
        in_specs=[anywhere] * 18,
        out_specs=(vmem, vmem),
        scratch_shapes=[
            pltpu.VMEM((tokens, width), bf16),
            pltpu.VMEM((1, width), f32),
            pltpu.VMEM((top_count, tokens), jnp.int32),
            pltpu.VMEM((top_count, tokens), f32),
            pltpu.VMEM((1, wide), f32),
            pltpu.VMEM((6, length, wide), bf16),
            pltpu.VMEM((wide, 2 * wide), f32),
            pltpu.VMEM((length, wide), f32),
            pltpu.VMEM((length, wide), f32),
            pltpu.VMEM((length, wide), bf16),
            pltpu.VMEM((groups, 2, HEAD_DIM, wide), bf16),
            pltpu.VMEM((tokens, peers * wide), bf16),
            pltpu.VMEM((peers * wide, width), bf16),
            pltpu.VMEM((2 * local, 4 * height, width), bf16),
            pltpu.VMEM((local, 4 * height, width), bf16),
            pltpu.VMEM(shared_gate.shape, bf16),
            pltpu.VMEM(shared_up.shape, bf16),
            pltpu.VMEM(shared_down.shape, bf16),
            pltpu.VMEM((tokens, inner), bf16),
            pltpu.VMEM((tokens, width), f32),
            pltpu.VMEM((teams, tokens, width), bf16),
            pltpu.VMEM((teams, top_count, tokens), jnp.int32),
            pltpu.VMEM((teams, top_count, tokens), f32),
            pltpu.VMEM((tokens, width), bf16),
            pltpu.VMEM((experts * slots, tokens), bf16),
            pltpu.VMEM((teams, tokens, experts * slots), bf16),
            pltpu.VMEM((teams, groups, span, width), bf16),
            pltpu.VMEM((teams, groups, span, width), bf16),
            pltpu.VMEM((teams, groups, span, width), bf16),
            pltpu.VMEM((teams, local, groups * slots, 4 * height), bf16),
            pltpu.VMEM((teams, tokens, width), bf16),
            pltpu.VMEM((teams, tokens, width), bf16),
            dma((teams, 2)),
            dma((teams, 2)),
            dma((teams, pieces)),
            dma((teams, pieces)),
            dma((teams,)),
            dma((teams,)),
            dma((teams, groups)),
            dma((teams, groups)),
            dma((cuts + teams,)),
            dma((cuts + teams,)),
            dma((cuts + teams,)),
            dma((cuts + teams,)),
            dma((cuts + teams,)),
            dma((cuts + teams,)),
            dma((cuts + 5,)),
            dma((11,)),
            dma((teams,)),
            dma((teams,)),
            dma((teams,)),
            dma((teams, pieces)),
            dma((teams, pieces)),
            dma((teams, pieces)),
            dma((groups,)),
            dma((groups,)),
            dma((peers,)),
            dma((peers,)),
        ],
        compiler_params=pltpu.CompilerParams(
            collective_id=0, has_side_effects=True, vmem_limit_bytes=62 << 20
        ),
    )(
        pad(norm_gain).reshape(1, wide),
        moe_in,
        moe_gain.reshape(1, width),
        routes.T,
        route_weights.T,
        pad(receptance),
        pad(key_in),
        pad(payload_vectors),
        pad(decay_in),
        pad(rate_in),
        pad(gate_in),
        weight_rows,
        turned(expert_gate),
        turned(expert_up),
        turned(expert_down),
        shared_gate,
        shared_up,
        shared_down,
    )


def solution(mesh):
    placed = (
        P("ep", "tp"),
        P("ep", "tp"),
        P("ep", "tp"),
        P("ep", "tp"),
        P("ep", "tp"),
        P("ep", "tp"),
        P("tp"),
        P("tp", None),
        P(("ep", "tp"), None),
        P(),
        P(("ep", "tp"), None),
        P(("ep", "tp"), None),
        P("ep", None, "tp"),
        P("ep", None, "tp"),
        P("ep", None, "tp"),
        P(),
        P(),
        P(),
    )
    return jax.shard_map(
        shards,
        mesh=mesh,
        in_specs=placed,
        out_specs=(P(("ep", "tp"), None), P(("ep", "tp"), None)),
        check_vma=False,
    )
```
